32 devices in a mesh: sp: 16 (over z, y, core), tp: 2 (over x).
Axes of the slice: x: 2, y: 2, z: 4, core: 2. Of those that a mesh axis runs over, the one named last changes fastest.
Arguments:
- asking_matrix: bfloat16 [2048, 2048], P('sp', 'tp'), may hold values from -30 to 30
- matching_key_matrix: bfloat16 [2048, 1024], P('sp', 'tp'), may hold values from -30 to 30
- carried_value_matrix: bfloat16 [2048, 1024], P('sp', 'tp'), may hold values from -48 to 48
- silu_switch_argument: bfloat16 [2048, 2048], P('sp', 'tp'), may hold values from -6 to 6
- duality_source_matrix: bfloat16 [2048, 2048], P('sp', 'tp'), may hold values from -6 to 6
- storing_direction_matrix: bfloat16 [2048, 1024], P('sp', 'tp'), may hold values from -6 to 6
- fetching_direction_matrix: bfloat16 [2048, 1024], P('sp', 'tp'), may hold values from -6 to 6
- duality_kernel_coefficients: bfloat16 [5, 2048], P(None, 'tp'), may hold values from -2.5 to 2.5
- storing_kernel_coefficients: bfloat16 [5, 1024], P(None, 'tp'), may hold values from -2.5 to 2.5
- fetching_kernel_coefficients: bfloat16 [5, 1024], P(None, 'tp'), may hold values from -2.5 to 2.5
- raw_increment_lengths: float32 [2, 32, 2048], P(None, 'tp', 'sp'), may hold values from -5.5 to 5.5
- logarithmic_fading_speeds: float32 [2, 32], P(None, 'tp'), may hold values from -16 to -2.9
- token_fading_spikes: float32 [2, 32, 2048], P(None, 'tp', 'sp'), may hold values from -2.1 to 0
- absorber_score_vector: float32 [16], P('tp'), may hold values from 4 to 8
- cluster_scaling_factor: float32 [2048], P('tp'), may hold values from 0.1 to 1.9
- final_mapping_matrix: bfloat16 [2, 2048, 4096], P(None, 'tp', 'sp'), may hold values from -0.09375 to 0.09375
Outputs:
- mixed_out: bfloat16 [2048, 4096], P(('sp', 'tp'))
The draws below stay inside these ranges and needn't reach their ends.
All inputs are finite; a program needn't handle non-finite values.
Results may differ from the reference program's by a relative error of at most 0.014.
Values may be sent and summed in bfloat16 or wider, within the bound.
A program may use at most 128 MiB of HBM per device.

```python
import math
import jax
import jax.numpy as jnp
from jax import lax

D = 4096
HEADS = 16
KV_HEADS = 8
HEAD = 128
SSD_HEADS = 32
SSD_HEAD = 64
GROUPS = 8
STATE = 128
CONV = 5
WINDOW = 128
SPAN = 128
TOK_DEV = 128
TOKENS = 2048
ATTN_W = 2048
KV_W = 1024
SSD_W = 2048
N_TP = 2


def drawn_rows(key):
    query_base = jnp.clip(jax.random.normal(jax.random.fold_in(key, 11), (TOKENS, ATTN_W), jnp.float32), -4.0, 4.0)
    key_base = jnp.clip(jax.random.normal(jax.random.fold_in(key, 12), (TOKENS, KV_W), jnp.float32), -4.0, 4.0)
    return (query_base, key_base)


def draw_asking_matrix(key, part):
    return drawn_rows(key)[0].astype(jnp.bfloat16)


def draw_matching_key_matrix(key, part):
    return drawn_rows(key)[1].astype(jnp.bfloat16)


def draw_raw_increment_lengths(key, part):
    jitter = jnp.clip(jax.random.normal(jax.random.fold_in(key, 21), (2, SSD_HEADS, TOKENS), jnp.float32), -4.0, 4.0)
    block_level = jax.random.uniform(jax.random.fold_in(key, 22), (2, SSD_HEADS, TOKENS // TOK_DEV), jnp.float32, -1.5, 1.5)
    return jitter + jnp.repeat(block_level, TOK_DEV, axis=2)


def draw_logarithmic_fading_speeds(key, part):
    keep_count = SSD_HEADS // 2
    ranking = jnp.stack([jax.random.permutation(jax.random.fold_in(key, 31), SSD_HEADS), jax.random.permutation(jax.random.fold_in(key, 32), SSD_HEADS)])
    lasting = ranking < keep_count
    slow_rate = jnp.exp(jax.random.uniform(jax.random.fold_in(key, 33), (2, SSD_HEADS), jnp.float32, math.log(0.02), math.log(0.3))) / TOKENS
    fast_rate = jnp.exp(jax.random.uniform(jax.random.fold_in(key, 34), (2, SSD_HEADS), jnp.float32, math.log(1.0 / 70.0), math.log(1.0 / 20.0)))
    return jnp.log(jnp.where(lasting, slow_rate, fast_rate))


def draw_token_fading_spikes(key, part):
    positions = jax.random.randint(jax.random.fold_in(key, 41), (2, SSD_HEADS, 3), 0, TOKENS)
    depths = jax.random.uniform(jax.random.fold_in(key, 42), (2, SSD_HEADS, 3), jnp.float32, 0.22, 0.69)
    places = jnp.arange(TOKENS, dtype=jnp.int32)
    hits = jnp.where(places[None, None, None, :] == positions[..., None], depths[..., None], 0.0)
    return -jnp.sum(hits, axis=2)


def block_levels(rng, dims, shards, smallest, top_value):
    loudness, own = 1.0, jax.random.fold_in(rng, 6)
    for position, blocks in shards:
        heights = jnp.exp(jax.random.uniform(jax.random.fold_in(own, position), (blocks,), jnp.float32, smallest / len(shards), top_value / len(shards)))
        loudness = loudness * jnp.repeat(heights, dims[position] // blocks).reshape([-1 if axis == position else 1 for axis in range(len(dims))])
    return loudness


def noise(stream_key, shape, scale, most, split=(), held_as=jnp.bfloat16):
    gain = block_levels(stream_key, shape, split, -0.22, 0.18) if split else 1.0
    values = jax.random.normal(stream_key, shape, jnp.float32) * scale * gain
    return jnp.minimum(jnp.maximum(values, -most), most).astype(held_as)


def setup_inputs(seed: int = 0) -> dict:
    key_of = jax.random.split(jax.random.key(seed), 17)
    asking_matrix = draw_asking_matrix(jax.random.fold_in(key_of[16], 71), 0)
    matching_key_matrix = draw_matching_key_matrix(jax.random.fold_in(key_of[16], 71), 0)
    carried_value_matrix = noise(key_of[2], (TOKENS, KV_W), 8.0, 48.0, ((0, 16), (1, 2)))
    silu_switch_argument = noise(key_of[3], (TOKENS, SSD_W), 1.0, 6.0, ((0, 16), (1, 2)))
    duality_source_matrix = noise(key_of[4], (TOKENS, SSD_W), 1.0, 6.0, ((0, 16), (1, 2)))
    storing_direction_matrix = noise(key_of[5], (TOKENS, GROUPS * STATE), 1.0, 6.0, ((0, 16), (1, 2)))
    fetching_direction_matrix = noise(key_of[6], (TOKENS, GROUPS * STATE), 1.0, 6.0, ((0, 16), (1, 2)))
    duality_kernel_coefficients = noise(key_of[7], (CONV, SSD_W), CONV ** -0.5, 2.5, ((1, 2),))
    storing_kernel_coefficients = noise(key_of[8], (CONV, GROUPS * STATE), CONV ** -0.5, 2.5, ((1, 2),))
    fetching_kernel_coefficients = noise(key_of[9], (CONV, GROUPS * STATE), CONV ** -0.5, 2.5, ((1, 2),))
    raw_increment_lengths = draw_raw_increment_lengths(jax.random.fold_in(key_of[16], 71), 0)
    logarithmic_fading_speeds = draw_logarithmic_fading_speeds(jax.random.fold_in(key_of[16], 71), 0)
    token_fading_spikes = draw_token_fading_spikes(jax.random.fold_in(key_of[16], 71), 0)
    absorber_score_vector = jnp.clip(4.0 + 4.0 * jax.random.uniform(key_of[13], (HEADS,), jnp.float32) ** block_levels(key_of[13], (HEADS,), ((0, 2),), -0.2, 0.2), 4.0, 8.0)
    cluster_scaling_factor = jnp.clip(1.0 + 0.18 * jax.random.normal(key_of[14], (SSD_W,), jnp.float32), 0.1, 1.9)
    final_mapping_matrix = noise(key_of[15], (2, ATTN_W, D), (2 * ATTN_W) ** -0.5, 0.09375, ((1, 2), (2, 16)))
    return {"asking_matrix": asking_matrix, "matching_key_matrix": matching_key_matrix, "carried_value_matrix": carried_value_matrix, "silu_switch_argument": silu_switch_argument, "duality_source_matrix": duality_source_matrix, "storing_direction_matrix": storing_direction_matrix, "fetching_direction_matrix": fetching_direction_matrix, "duality_kernel_coefficients": duality_kernel_coefficients, "storing_kernel_coefficients": storing_kernel_coefficients, "fetching_kernel_coefficients": fetching_kernel_coefficients, "raw_increment_lengths": raw_increment_lengths, "logarithmic_fading_speeds": logarithmic_fading_speeds, "token_fading_spikes": token_fading_spikes, "absorber_score_vector": absorber_score_vector, "cluster_scaling_factor": cluster_scaling_factor, "final_mapping_matrix": final_mapping_matrix}


ROTARY_BASE = 500000.0
EPSILON = 1e-06

def rotate(matrix, offset):
    row_count = matrix.shape[0]
    halfway = HEAD // 2
    heads_here = matrix.shape[1] // HEAD
    spacing = ROTARY_BASE ** (-jnp.arange(halfway, dtype=jnp.float32) * 2.0 / HEAD)
    places = (offset + jnp.arange(row_count, dtype=jnp.int32)).astype(jnp.float32)
    angles = places[:, None] * spacing[None, :]
    cosine = jnp.cos(angles)[:, None, :]
    sine_table = jnp.sin(angles)[:, None, :]
    halves = matrix.astype(jnp.float32).reshape(row_count, heads_here, 2, halfway)
    former = halves[:, :, 0]
    latter = halves[:, :, 1]
    turned = jnp.stack([former * cosine - latter * sine_table, latter * cosine + former * sine_table], axis=2)
    return turned.reshape(row_count, heads_here * HEAD).astype(jnp.bfloat16)

def attend(turned_queries, turned_keys, carried_value_matrix, absorber_score_vector):
    sharing = HEADS // KV_HEADS
    block_count = TOKENS // SPAN
    filler = jnp.zeros((SPAN, KV_W), jnp.bfloat16)
    key_pad = jnp.concatenate([filler, turned_keys, filler], axis=0)
    value_pad = jnp.concatenate([filler, carried_value_matrix, filler], axis=0)
    within = jnp.arange(SPAN, dtype=jnp.int32)[:, None]
    across = jnp.arange(3 * SPAN, dtype=jnp.int32)[None, :]
    inside = jnp.abs(across - SPAN - within) <= WINDOW
    sink_rows = absorber_score_vector.reshape(KV_HEADS, sharing)[:, :, None, None]

    def one_block(block_index):
        first_row = (block_index * SPAN).astype(jnp.int32)
        query_tile = lax.dynamic_slice_in_dim(turned_queries, first_row, SPAN, 0).reshape(SPAN, KV_HEADS, sharing, HEAD)
        key_tile = lax.dynamic_slice_in_dim(key_pad, first_row, 3 * SPAN, 0).reshape(3 * SPAN, KV_HEADS, HEAD)
        value_tile = lax.dynamic_slice_in_dim(value_pad, first_row, 3 * SPAN, 0).reshape(3 * SPAN, KV_HEADS, HEAD)
        places = first_row - SPAN + across
        allowed = inside & (places >= 0) & (places < TOKENS)
        scores = jnp.einsum('qkgd,skd->kgqs', query_tile.astype(jnp.float32), key_tile.astype(jnp.float32)) * HEAD ** (-0.5)
        scores = jnp.where(allowed, scores, -jnp.inf)
        ceiling = jnp.maximum(lax.optimization_barrier(jnp.max(scores, axis=-1, keepdims=True)), sink_rows)
        weights = jnp.exp(scores - ceiling)
        denominator = lax.optimization_barrier(jnp.sum(weights, axis=-1, keepdims=True)) + jnp.exp(sink_rows - ceiling)
        probabilities = (weights / denominator).astype(jnp.bfloat16)
        attended = jnp.einsum('kgqs,skd->qkgd', probabilities.astype(jnp.float32), value_tile.astype(jnp.float32))
        return attended.reshape(SPAN, ATTN_W).astype(jnp.bfloat16)
    return lax.map(one_block, jnp.arange(block_count, dtype=jnp.int32)).reshape(TOKENS, ATTN_W)

def convolve(padded, taps_all, row_count):
    summed = jnp.zeros((row_count, padded.shape[1]), jnp.float32)
    for tap_index in range(CONV):
        summed = summed + padded[tap_index:tap_index + row_count].astype(jnp.float32) * taps_all[tap_index].astype(jnp.float32)
    return jax.nn.silu(summed).astype(jnp.bfloat16)

def sweep(scan_rows, step_rows, decay_rows, write_rows, read_rows):
    per_group = SSD_HEADS // GROUPS
    block_count = TOKENS // SPAN
    highest = lax.Precision.HIGHEST
    scan_tiles = scan_rows.reshape(block_count, SPAN, GROUPS, per_group, SSD_HEAD)
    step_tiles = step_rows.reshape(block_count, SPAN, GROUPS, per_group)
    decay_tiles = decay_rows.reshape(block_count, SPAN, GROUPS, per_group)
    write_tiles = write_rows.reshape(block_count, SPAN, GROUPS, STATE)
    read_tiles = read_rows.reshape(block_count, SPAN, GROUPS, STATE)
    earlier_mask = jnp.arange(SPAN)[:, None] >= jnp.arange(SPAN)[None, :]

    def advance(carried, block_item):
        scan_tile, step_tile, decay_tile, write_tile, read_tile = block_item
        scaled = scan_tile.astype(jnp.float32) * step_tile[..., None]
        write_values = write_tile.astype(jnp.float32)
        read_values = read_tile.astype(jnp.float32)
        running = jnp.cumsum(decay_tile, axis=0)
        spread = running[:, None] - running[None, :]
        fading = jnp.exp(jnp.where(earlier_mask[:, :, None, None], spread, -jnp.inf))
        affinity = jnp.einsum('lgn,sgn->lsg', read_values, write_values, precision=highest)
        within_block = jnp.einsum('lsgr,sgrp->lgrp', affinity[..., None] * fading, scaled, precision=highest)
        from_before = jnp.einsum('lgn,grpn->lgrp', read_values, carried, precision=highest) * jnp.exp(running)[..., None]
        to_end = jnp.exp(running[-1:] - running)
        block_states = jnp.einsum('lgn,lgrp->grpn', write_values, scaled * to_end[..., None], precision=highest)
        return (carried * jnp.exp(running[-1])[..., None, None] + block_states, within_block + from_before)
    start_state = jnp.zeros((GROUPS, per_group, SSD_HEAD, STATE), jnp.float32)
    final_state, outputs = lax.scan(advance, start_state, (scan_tiles, step_tiles, decay_tiles, write_tiles, read_tiles))
    return outputs.reshape(TOKENS, SSD_W)

def reference(asking_matrix, matching_key_matrix, carried_value_matrix, silu_switch_argument, duality_source_matrix, storing_direction_matrix, fetching_direction_matrix, duality_kernel_coefficients, storing_kernel_coefficients, fetching_kernel_coefficients, raw_increment_lengths, logarithmic_fading_speeds, token_fading_spikes, absorber_score_vector, cluster_scaling_factor, final_mapping_matrix):
    attended = attend(rotate(asking_matrix, 0), rotate(matching_key_matrix, 0), carried_value_matrix, absorber_score_vector)
    margin = CONV // 2
    raw_rows = jnp.concatenate([duality_source_matrix, storing_direction_matrix, fetching_direction_matrix], axis=1)
    padded = jnp.pad(raw_rows, ((margin, margin), (0, 0)))
    conved = convolve(padded, jnp.concatenate([duality_kernel_coefficients, storing_kernel_coefficients, fetching_kernel_coefficients], axis=1), TOKENS)
    per_group = SSD_HEADS // GROUPS
    scan_rows = conved[:, :SSD_W].reshape(TOKENS, GROUPS, per_group, SSD_HEAD)
    write_rows = conved[:, SSD_W:SSD_W + GROUPS * STATE].reshape(TOKENS, GROUPS, STATE)
    read_rows = conved[:, SSD_W + GROUPS * STATE:].reshape(TOKENS, GROUPS, STATE)
    joint_increment_lengths = jax.nn.softplus(raw_increment_lengths)
    joint_fading_amounts = -jnp.exp(logarithmic_fading_speeds)[:, :, None] * joint_increment_lengths + token_fading_spikes
    steps_rows = jnp.transpose(joint_increment_lengths, (0, 2, 1)).reshape(2, TOKENS, GROUPS, per_group)
    decay_rows = jnp.transpose(joint_fading_amounts, (0, 2, 1)).reshape(2, TOKENS, GROUPS, per_group)
    ahead_rows = sweep(scan_rows, steps_rows[0], decay_rows[0], write_rows, read_rows)
    back_rows = sweep(scan_rows[::-1], steps_rows[1][::-1], decay_rows[1][::-1], write_rows[::-1], read_rows[::-1])[::-1]
    gated_rows = (ahead_rows + back_rows) * jax.nn.silu(silu_switch_argument.astype(jnp.float32))
    grouped = gated_rows.reshape(TOKENS, GROUPS, SSD_W // GROUPS)
    grouped = grouped * lax.rsqrt(lax.optimization_barrier(jnp.mean(grouped * grouped, axis=-1, keepdims=True)) + EPSILON)
    normed = (grouped.reshape(TOKENS, SSD_W) * cluster_scaling_factor).astype(jnp.bfloat16)
    slice_width = ATTN_W // N_TP
    summed = jnp.zeros((TOKENS, D), jnp.float32)
    for shard_index in range(N_TP):
        first_col = shard_index * slice_width
        partial_sum = jnp.dot(attended[:, first_col:first_col + slice_width], final_mapping_matrix[0, first_col:first_col + slice_width], preferred_element_type=jnp.float32)
        partial_sum = partial_sum + jnp.dot(normed[:, first_col:first_col + slice_width], final_mapping_matrix[1, first_col:first_col + slice_width], preferred_element_type=jnp.float32)
        rounded = lax.optimization_barrier(partial_sum.astype(jnp.bfloat16))
        summed = summed + rounded.astype(jnp.float32)
    return summed.astype(jnp.bfloat16)
```

```python
import functools

import jax
import jax.numpy as jnp
from jax import lax
from jax.experimental import pallas as pl
from jax.experimental.pallas import tpu as pltpu
from jax.sharding import PartitionSpec as P

HEAD = 128
SSD_HEAD = 64
STATE = 128
CONV = 5
WINDOW = 128
CLIQUE = 4
TILE = 16
LANES = 128
CHUNKS = 4
PARTS = 4
EARLY = 3

ROTARY_BASE = 500000.0
EPSILON = 1e-06

F32 = jnp.float32
BF16 = jnp.bfloat16


def sending(source, target, send_sem, recv_sem, partner):
    return pltpu.make_async_remote_copy(
        src_ref=source,
        dst_ref=target,
        send_sem=send_sem,
        recv_sem=recv_sem,
        device_id=partner,
        device_id_type=pl.DeviceIdType.MESH,
    )


def dot(a, b):
    return jnp.dot(a, b, preferred_element_type=F32)


def dot_t(a, b):
    return lax.dot_general(a, b, (((1,), (1,)), ((), ())), preferred_element_type=F32)


def iota(shape, axis):
    return lax.broadcasted_iota(jnp.int32, shape, axis)


def silu(v):
    return v / (1.0 + jnp.exp(-v))


def split(value):
    high = value.astype(BF16)
    return high, (value - high.astype(F32)).astype(BF16)


def mixer_kernel(
    outer,
    tps,
    q_ref,
    k_ref,
    v_ref,
    gate_ref,
    src_ref,
    wr_ref,
    rd_ref,
    src_taps,
    wr_taps,
    rd_taps,
    inc_ref,
    fade_ref,
    spike_ref,
    sink_ref,
    gain_ref,
    weight_ref,
    cos_ref,
    sin_ref,
    out_ref,
    turned,
    k_halo,
    v_halo,
    src_halo,
    wr_halo,
    rd_halo,
    padded,
    xs,
    wv,
    rv,
    square,
    grown,
    scaled,
    rows_log,
    logs,
    decays,
    own_state,
    state_out,
    mate_state,
    total,
    total_out,
    partner_total,
    z_out,
    z_in,
    chip_out,
    incoming,
    y_sum,
    acts,
    weights,
    acc,
    partial,
    pieces,
    summed,
    landed,
    halo_sems,
    log_sems,
    weight_sems,
    scan_sems,
    act_sems,
    own_sems,
    piece_sems,
    out_sems,
    load_sem,
):
    count = outer * CLIQUE
    rows = q_ref.shape[0]
    me = lax.axis_index("sp")
    lane = lax.axis_index("tp")
    spot = lax.rem(me, CLIQUE)
    layer = me // CLIQUE
    base = me - spot
    core = lax.rem(spot, 2)
    side_y = spot // 2
    mate = base + spot + 1 - 2 * core
    partner = base + lax.rem(spot + 2, CLIQUE)
    across = base + CLIQUE - 1 - spot
    way = 1 - core
    step = 1 - 2 * way
    before = layer - step
    after = layer + step
    has_before = (before >= 0) & (before < outer)
    has_after = (after >= 0) & (after < outer)
    later = (side_y + way) == 1
    has_left = me > 0
    has_right = me < count - 1
    left = {"sp": me - 1}
    right = {"sp": me + 1}

    def at_layer(other):
        return {"sp": other * CLIQUE + spot}

    barrier = pltpu.get_barrier_semaphore()

    def hail(who):
        pl.semaphore_signal(
            barrier, inc=1, device_id=who, device_id_type=pl.DeviceIdType.MESH
        )

    for other in (mate, partner, across):
        hail({"sp": other})
    for d in range(1, outer):
        hail(at_layer(lax.rem(layer + d, outer)))
    for d in range(1, tps):
        hail({"tp": lax.rem(lane + d, tps)})
    extra_right = (spot == CLIQUE - 1) & has_right
    extra_left = (spot == 0) & has_left
    pl.when(extra_right)(lambda: hail(right))
    pl.when(extra_left)(lambda: hail(left))
    hails = CLIQUE - 1 + outer - 1 + tps - 1
    load = pltpu.make_async_copy(weight_ref, weights.at[spot], load_sem)
    load.start()

    cosine = cos_ref[...]
    sine = sin_ref[...]

    def turn(block):
        block = block.astype(F32)
        return (block * cosine + pltpu.roll(block, HEAD // 2, 1) * sine).astype(BF16)

    kv_heads = k_ref.shape[1] // HEAD
    for g in range(kv_heads):
        cols = slice(g * HEAD, (g + 1) * HEAD)
        turned[:, cols] = turn(k_ref[:, cols])

    heads = inc_ref.shape[1]
    gap = LANES // 4
    lane_at = iota((heads, rows), 1)
    eye = iota((heads, heads), 0) == iota((heads, heads), 1)
    steps = []
    runs = []
    for d in range(2):
        raw = inc_ref[d]
        length = jnp.maximum(raw, 0.0) + jnp.log1p(jnp.exp(-jnp.abs(raw)))
        rate = jnp.sum(
            jnp.where(eye, jnp.broadcast_to(jnp.exp(fade_ref[d : d + 1, :]), (heads, heads)), 0.0),
            axis=1,
            keepdims=True,
        )
        run = spike_ref[d] - rate * length
        hop = 1
        while hop < rows:
            if d == 0:
                moved = jnp.where(lane_at >= hop, pltpu.roll(run, hop, 1), 0.0)
            else:
                moved = jnp.where(lane_at < rows - hop, pltpu.roll(run, rows - hop, 1), 0.0)
            run = run + moved
            hop *= 2
        steps.append(length)
        runs.append(run)
    ends = [runs[0][:, rows - 1 : rows], runs[1][:, 0:1]]
    square[...] = jnp.zeros_like(square)
    for d in range(2):
        square[0, d * gap : d * gap + heads, :] = runs[d]
        fill = jnp.exp(runs[d])
        high = fill.astype(BF16).astype(F32)
        square[1, 2 * d * gap : 2 * d * gap + heads, :] = high
        square[1, (2 * d + 1) * gap : (2 * d + 1) * gap + heads, :] = fill - high
        fill = steps[d] * jnp.exp(ends[d] - runs[d])
        high = fill.astype(BF16).astype(F32)
        square[2, 2 * d * gap : 2 * d * gap + heads, :] = high
        square[2, (2 * d + 1) * gap : (2 * d + 1) * gap + heads, :] = fill - high
        rows_log[d] = runs[d]
        rows_log[2 + d] = steps[d]
    run_cols = square[0].T
    log_row = iota((8, LANES), 0)
    logs[spot] = jnp.where(
        log_row == 0,
        jnp.broadcast_to(run_cols[rows - 1 : rows, :], (8, LANES)),
        jnp.broadcast_to(run_cols[0:1, :], (8, LANES)),
    )

    def when_wait(ready):
        pl.semaphore_wait(barrier, ready)

    when_wait(
        hails + extra_right.astype(jnp.int32) + extra_left.astype(jnp.int32)
    )

    rims = (
        (src_ref, src_halo, TILE),
        (wr_ref, wr_halo, TILE),
        (rd_ref, rd_halo, TILE),
        (turned, k_halo, rows),
        (v_ref, v_halo, rows),
    )

    def rim_copy(index, to_right):
        source, target, depth = rims[index]
        side = 0 if to_right else 1
        first = rows - depth if to_right else 0
        return sending(
            source.at[first : first + depth, :],
            target.at[side],
            halo_sems.at[0, side, index],
            halo_sems.at[1, side, index],
            right if to_right else left,
        )

    def rims_do(indices, what):
        for index in indices:
            if what == "start":
                pl.when(has_right)(lambda: rim_copy(index, True).start())
                pl.when(has_left)(lambda: rim_copy(index, False).start())
            elif what == "recv":
                pl.when(has_left)(lambda: rim_copy(index, True).wait_recv())
                pl.when(has_right)(lambda: rim_copy(index, False).wait_recv())
            else:
                pl.when(has_right)(lambda: rim_copy(index, True).wait_send())
                pl.when(has_left)(lambda: rim_copy(index, False).wait_send())

    rims_do(range(5), "start")

    def clear(side):
        for _, target, _ in rims:
            target[side] = jnp.zeros(target.shape[1:], target.dtype)

    pl.when(jnp.logical_not(has_left))(lambda: clear(0))
    pl.when(jnp.logical_not(has_right))(lambda: clear(1))

    def clear_in():
        z_in[...] = jnp.zeros_like(z_in)

    pl.when(jnp.logical_not(has_before))(clear_in)

    def log_copy(flip, who, slot):
        return sending(
            logs.at[slot],
            logs.at[slot],
            log_sems.at[0, flip],
            log_sems.at[1, flip],
            {"sp": base + who},
        )

    flips = (
        spot + 1 - 2 * core,
        lax.rem(spot + 2, CLIQUE),
        CLIQUE - 1 - spot,
    )
    for flip, who in enumerate(flips):
        log_copy(flip, who, spot).start()

    load.wait()
    depth = weights.shape[2] // PARTS

    def weight_part(slot, index):
        half, part = divmod(index, PARTS)
        return weights.at[slot, half, part * depth : (part + 1) * depth, :]

    def weight_mate(half, slot):
        return sending(
            weights.at[slot, half],
            weights.at[slot, half],
            weight_sems.at[0, 0, half],
            weight_sems.at[1, 0, half],
            {"sp": mate},
        )

    def weight_over(index, slot):
        return sending(
            weight_part(slot, index),
            weight_part(slot, index),
            weight_sems.at[0, 1, index],
            weight_sems.at[1, 1, index],
            {"sp": partner},
        )

    def weight_onward(index, slot):
        return sending(
            weight_part(slot, index),
            weight_part(slot, index),
            weight_sems.at[0, 2, index],
            weight_sems.at[1, 2, index],
            {"sp": mate},
        )

    def pass_on(index):
        weight_over(index, flips[1]).wait_recv()
        weight_onward(index, flips[1]).start()

    for index in range(EARLY):
        weight_over(index, spot).start()
    for half in range(2):
        weight_mate(half, spot).start()

    rims_do(range(3), "recv")
    columns = ((src_ref, src_halo, src_taps, xs), (wr_ref, wr_halo, wr_taps, wv), (rd_ref, rd_halo, rd_taps, rv))
    margin = CONV // 2
    for source, halo, taps_ref, target in columns:
        width = source.shape[1]
        taps = taps_ref[...].astype(F32)
        for first in range(0, width, LANES):
            cols = slice(first, first + LANES)
            padded[8 : 8 + rows, :] = source[:, cols].astype(F32)
            padded[0:8, :] = halo[0, TILE // 2 :, cols].astype(F32)
            padded[8 + rows : 16 + rows, :] = halo[1, : TILE // 2, cols].astype(F32)
            value = jnp.zeros((rows, LANES), F32)
            for k in range(CONV):
                start = 8 - margin + k
                value = value + padded[start : start + rows, :] * taps[k : k + 1, cols]
            target[:, cols] = silu(value).astype(BF16)

    rims_do(range(3, 5), "recv")
    sharing = q_ref.shape[1] // HEAD // kv_heads
    above = iota((rows, rows), 1) >= iota((rows, rows), 0)
    below = iota((rows, rows), 1) <= iota((rows, rows), 0)
    ok_left = above & has_left
    ok_right = below & has_right
    scale = HEAD ** (-0.5)
    for g in range(kv_heads):
        cols = slice(g * HEAD, (g + 1) * HEAD)
        keys = (k_halo[0, :, cols], turned[:, cols], k_halo[1, :, cols])
        values = (v_halo[0, :, cols], v_ref[:, cols], v_halo[1, :, cols])
        for j in range(sharing):
            h = g * sharing + j
            mine = slice(h * HEAD, (h + 1) * HEAD)
            query = turn(q_ref[:, mine])
            tiles = [dot_t(query, key) * scale for key in keys]
            tiles[0] = jnp.where(ok_left, tiles[0], -jnp.inf)
            tiles[2] = jnp.where(ok_right, tiles[2], -jnp.inf)
            sink = sink_ref[h]
            top = jnp.maximum(
                jnp.max(
                    jnp.maximum(jnp.maximum(tiles[0], tiles[1]), tiles[2]), axis=1, keepdims=True
                ),
                sink,
            )
            tiles = [jnp.exp(tile - top) for tile in tiles]
            bottom = jnp.sum(tiles[0] + tiles[1] + tiles[2], axis=1, keepdims=True) + jnp.exp(
                sink - top
            )
            found = jnp.zeros((rows, HEAD), F32)
            for tile, value in zip(tiles, values):
                found = found + dot((tile / bottom).astype(BF16), value)
            acts[0, layer, :, mine] = found.astype(BF16)

    def own_copy(half, way_up):
        target = layer + (1 if way_up else -1)
        return sending(
            acts.at[half, layer],
            acts.at[half, layer],
            own_sems.at[half, 1 if way_up else 0],
            act_sems.at[1, half, layer],
            at_layer(target),
        )

    can_up = layer < outer - 1
    can_down = layer > 0

    def own_start(half):
        pl.when(can_up)(lambda: own_copy(half, True).start())
        pl.when(can_down)(lambda: own_copy(half, False).start())

    def far_copy(half, block, sign):
        return sending(
            acts.at[half, block],
            acts.at[half, block],
            act_sems.at[0, half, block],
            act_sems.at[1, half, block],
            at_layer(layer - sign),
        )

    def each(d, do):
        for sign in (-1, 1):
            block = layer + sign * d
            pl.when((block >= 0) & (block < outer))(functools.partial(do, block, sign))

    def relay(half, d):
        def do(block, sign):
            copy = far_copy(half, block, sign)
            copy.wait_recv()
            target = layer - sign
            pl.when((target >= 0) & (target < outer))(lambda: copy.start())

        each(d, do)

    own_start(0)

    groups = wr_ref.shape[1] // STATE
    wide = xs.shape[1]
    group_wide = wide // groups
    per_group = group_wide // SSD_HEAD
    owner = iota((LANES, wide), 1) // SSD_HEAD
    place = iota((LANES, wide), 0)
    pick = []
    for d in range(2):
        hit = (place == owner + 2 * d * gap) | (place == owner + (2 * d + 1) * gap)
        pick.append(jnp.where(hit, 1.0, 0.0).astype(BF16))
    grow_cols = square[1].T.astype(BF16)
    scale_cols = square[2].T.astype(BF16)
    for d in range(2):
        grown[d] = dot(grow_cols, pick[d])
        scaled[d] = (dot(scale_cols, pick[d]) * xs[...].astype(F32)).astype(BF16)
    for g in range(groups):
        cols = slice(g * group_wide, (g + 1) * group_wide)
        write_t = wv[:, g * STATE : (g + 1) * STATE].astype(F32).T.astype(BF16)
        for d in range(2):
            fresh = dot(write_t, scaled[d, :, cols])
            own_state[d, :, cols] = fresh
            state_out[d, :, cols] = fresh.astype(BF16)

    swap = sending(
        state_out.at[1 - way],
        mate_state,
        scan_sems.at[0, 0, 0],
        scan_sems.at[1, 0, 0],
        {"sp": mate},
    )
    swap.start()

    for flip, who in enumerate(flips):
        log_copy(flip, who, who).wait_recv()
    log_own = logs[spot, pl.ds(way, 1), :]
    log_mate = logs[flips[0], pl.ds(way, 1), :]
    log_partner = logs[flips[1], pl.ds(way, 1), :] + logs[flips[2], pl.ds(way, 1), :]
    log_rows = jnp.where(
        log_row == 0,
        jnp.broadcast_to(log_own, (8, LANES)),
        jnp.where(
            log_row == 1,
            jnp.broadcast_to(log_mate, (8, LANES)),
            jnp.where(
                log_row == 2,
                jnp.broadcast_to(log_partner, (8, LANES)),
                jnp.broadcast_to(log_own + log_mate, (8, LANES)),
            ),
        ),
    )
    high, low = split(jnp.exp(log_rows))
    mine = jnp.where(place == owner + way * gap, 1.0, 0.0).astype(BF16)
    decays[...] = dot(high, mine) + dot(low, mine)
    dec_own = decays[0:1, :]
    dec_mate = decays[1:2, :]
    dec_partner = decays[2:3, :]
    dec_chip = decays[3:4, :]
    dec_layer = dec_partner * dec_chip
    one = jnp.ones_like(dec_own)
    from_partner = jnp.where(later, dec_chip, one)
    from_mine = jnp.where(later, one, dec_partner)
    in_before = jnp.where(later, dec_partner, one)
    in_partner = jnp.where(later, 1.0, 0.0)

    chunk = STATE // CHUNKS

    def over_copy(c):
        part = slice(c * chunk, (c + 1) * chunk)
        return sending(
            total_out.at[part, :],
            partner_total.at[part, :],
            scan_sems.at[0, 1, c],
            scan_sems.at[1, 1, c],
            {"sp": partner},
        )

    def z_copy(c, to):
        part = slice(c * chunk, (c + 1) * chunk)
        return sending(
            z_out.at[part, :],
            z_in.at[part, :],
            scan_sems.at[0, 2, c],
            scan_sems.at[1, 2, c],
            at_layer(to),
        )

    def down_copy(c):
        part = slice(c * chunk, (c + 1) * chunk)
        return sending(
            chip_out.at[part, :],
            incoming.at[way, part, :],
            scan_sems.at[0, 3, c],
            scan_sems.at[1, 3, c],
            {"sp": mate},
        )

    def down_recv(c):
        part = slice(c * chunk, (c + 1) * chunk)
        return sending(
            chip_out.at[part, :],
            incoming.at[1 - way, part, :],
            scan_sems.at[0, 3, c],
            scan_sems.at[1, 3, c],
            {"sp": mate},
        )

    swap.wait_recv()
    for c in range(CHUNKS):
        part = slice(c * chunk, (c + 1) * chunk)
        summed_state = (
            mate_state[part, :].astype(F32) * dec_own + own_state[way, part, :]
        )
        total[part, :] = summed_state
        total_out[part, :] = summed_state.astype(BF16)
        over_copy(c).start()
    for index in range(EARLY, 2 * PARTS):
        weight_over(index, spot).start()

    run_at = square[0].T
    causal = iota((rows, rows), 1) <= iota((rows, rows), 0)
    diagonal = iota((rows, rows), 1) == iota((rows, rows), 0)

    def within(g):
        read = rv[:, g * STATE : (g + 1) * STATE]
        write = wv[:, g * STATE : (g + 1) * STATE]
        affinity = dot_t(read, write)
        for j in range(per_group):
            h = g * per_group + j
            cols = slice(h * SSD_HEAD, (h + 1) * SSD_HEAD)
            ahead = run_at[:, h : h + 1] - rows_log[0, h : h + 1, :]
            back = run_at[:, gap + h : gap + h + 1] - rows_log[1, h : h + 1, :]
            fade = jnp.exp(jnp.where(causal, ahead, back))
            length_f = rows_log[2, h : h + 1, :]
            length_b = rows_log[3, h : h + 1, :]
            taken = jnp.where(causal, length_f, length_b) * fade
            taken = taken + jnp.where(diagonal, length_b, 0.0)
            y_sum[:, cols] = dot((affinity * taken).astype(BF16), xs[:, cols])

    for g in range(groups):
        within(g)
    for index in range(EARLY):
        pass_on(index)

    for c in range(CHUNKS):
        part = slice(c * chunk, (c + 1) * chunk)
        over_copy(c).wait_recv()
        theirs = partner_total[part, :].astype(F32)
        level = theirs * from_partner + total[part, :] * from_mine
        pl.when(has_before)(lambda: z_copy(c, after).wait_recv())
        entering = z_in[part, :].astype(F32)
        z_out[part, :] = (entering * dec_layer + level).astype(BF16)
        pl.when(has_after)(lambda: z_copy(c, after).start())
        chip_in = entering * in_before + theirs * in_partner
        chip_out[part, :] = chip_in.astype(BF16)
        down_copy(c).start()
        incoming[way, part, :] = (
            chip_in * dec_mate + mate_state[part, :].astype(F32)
        ).astype(BF16)
    if outer > 1:
        relay(0, 1)
    for c in range(CHUNKS):
        down_recv(c).wait_recv()

    for g in range(groups):
        cols = slice(g * group_wide, (g + 1) * group_wide)
        read = rv[:, g * STATE : (g + 1) * STATE]
        value = y_sum[:, cols]
        for d in range(2):
            value = value + dot(read, incoming[d, :, cols]) * grown[d, :, cols]
        value = value * silu(gate_ref[:, cols].astype(F32))
        mean = jnp.sum(value * value, axis=1, keepdims=True) * (1.0 / group_wide)
        value = value * lax.rsqrt(mean + EPSILON) * gain_ref[:, cols]
        acts[1, layer, :, cols] = value.astype(BF16)
    own_start(1)

    share = rows // tps

    def multiply_first(block, sign):
        def body(slot, carry):
            acc[block, slot] = dot(acts[0, block], weights[slot, 0])
            return carry

        lax.fori_loop(0, CLIQUE, body, 0)

    def piece_copy(block, other, slot):
        return sending(
            partial.at[block, other],
            pieces.at[block, slot],
            piece_sems.at[0, block, other],
            piece_sems.at[1, block, slot],
            {"tp": other},
        )

    lanes = [lax.rem(lane + d, tps) for d in range(1, tps)]

    def multiply_second(block, sign):
        def body(slot, carry):
            product = (acc[block, slot] + dot(acts[1, block], weights[slot, 1])).astype(BF16)
            for other in range(tps):
                partial[block, other, slot] = product[other * share : (other + 1) * share]
            return carry

        lax.fori_loop(0, CLIQUE, body, 0)
        for other in lanes:
            piece_copy(block, other, lane).start()

    def out_copy(block, slot):
        return sending(
            summed.at[block],
            landed.at[slot],
            out_sems.at[0, block],
            out_sems.at[1, slot],
            at_layer(block),
        )

    def settle(block, sign):
        result = partial[block, lane].astype(F32)
        for other in lanes:
            piece_copy(block, other, other).wait_recv()
            result = result + pieces[block, other].astype(F32)
        if sign:
            summed[block] = result.astype(BF16)
            out_copy(block, layer).start()
        else:
            landed[layer] = result.astype(BF16)

    for index in range(EARLY, PARTS):
        pass_on(index)
    weight_mate(0, flips[0]).wait_recv()
    for index in range(PARTS):
        weight_onward(index, flips[2]).wait_recv()
    multiply_first(layer, 0)
    for d in range(1, outer):
        if d > 1:
            relay(0, d)
        each(d, multiply_first)
    for index in range(PARTS, 2 * PARTS):
        pass_on(index)
    weight_mate(1, flips[0]).wait_recv()
    for index in range(PARTS, 2 * PARTS):
        weight_onward(index, flips[2]).wait_recv()
    multiply_second(layer, 0)
    for d in range(1, outer):
        relay(1, d)
        each(d, multiply_second)
        if d == 1:
            settle(layer, 0)
        else:
            each(d - 1, settle)
    if outer > 1:
        each(outer - 1, settle)
    else:
        settle(layer, 0)

    def arrive(block, sign):
        out_copy(block, block).wait_recv()

    for d in range(1, outer):
        each(d, arrive)
    width = landed.shape[3]
    for other in range(outer):
        for slot in range(CLIQUE):
            first = (other * CLIQUE + slot) * width
            out_ref[:, first : first + width] = landed[other, slot]

    rims_do(range(5), "send")
    for flip, who in enumerate(flips):
        log_copy(flip, who, spot).wait_send()
    for half in range(2):
        weight_mate(half, spot).wait_send()
        pl.when(can_up)(lambda: own_copy(half, True).wait_send())
        pl.when(can_down)(lambda: own_copy(half, False).wait_send())
    for index in range(2 * PARTS):
        weight_over(index, spot).wait_send()
        weight_onward(index, flips[1]).wait_send()
    swap.wait_send()
    for c in range(CHUNKS):
        over_copy(c).wait_send()
        down_copy(c).wait_send()
        pl.when(has_after)(lambda: z_copy(c, after).wait_send())

    def gone(block, sign):
        target = layer - sign
        for half in range(2):
            pl.when((target >= 0) & (target < outer))(
                lambda: far_copy(half, block, sign).wait_send()
            )
        out_copy(block, layer).wait_send()
        for other in lanes:
            piece_copy(block, other, lane).wait_send()

    for d in range(1, outer):
        each(d, gone)
    for other in lanes:
        piece_copy(layer, other, lane).wait_send()


def local(
    asking_matrix,
    matching_key_matrix,
    carried_value_matrix,
    silu_switch_argument,
    duality_source_matrix,
    storing_direction_matrix,
    fetching_direction_matrix,
    duality_kernel_coefficients,
    storing_kernel_coefficients,
    fetching_kernel_coefficients,
    raw_increment_lengths,
    logarithmic_fading_speeds,
    token_fading_spikes,
    absorber_score_vector,
    cluster_scaling_factor,
    final_mapping_matrix,
):
    count = lax.axis_size("sp")
    tps = lax.axis_size("tp")
    outer = count // CLIQUE
    rows, q_width = asking_matrix.shape
    k_width = matching_key_matrix.shape[1]
    s_width = duality_source_matrix.shape[1]
    w_width = storing_direction_matrix.shape[1]
    heads = raw_increment_lengths.shape[1]
    width = final_mapping_matrix.shape[2]
    share = rows // tps
    halfway = HEAD // 2
    spacing = ROTARY_BASE ** (-jnp.arange(halfway, dtype=F32) * 2.0 / HEAD)
    places = (lax.axis_index("sp") * rows + jnp.arange(rows, dtype=jnp.int32)).astype(F32)
    angles = places[:, None] * jnp.concatenate([spacing, spacing])[None, :]
    sign = jnp.where(jnp.arange(HEAD) < halfway, -1.0, 1.0).astype(F32)
    cosine = jnp.cos(angles)
    sine = jnp.sin(angles) * sign[None, :]
    vmem = pl.BlockSpec(memory_space=pltpu.VMEM)
    block = (CLIQUE, share, width)
    return pl.pallas_call(
        functools.partial(mixer_kernel, outer, tps),
        out_shape=jax.ShapeDtypeStruct((share, count * width), BF16),
        in_specs=[vmem] * 13
        + [pl.BlockSpec(memory_space=pltpu.SMEM), vmem, pl.BlockSpec(memory_space=pl.ANY)]
        + [vmem] * 2,
        out_specs=vmem,
        scratch_shapes=[
            pltpu.VMEM((rows, k_width), BF16),
            pltpu.VMEM((2, rows, k_width), BF16),
            pltpu.VMEM((2, rows, k_width), BF16),
            pltpu.VMEM((2, TILE, s_width), BF16),
            pltpu.VMEM((2, TILE, w_width), BF16),
            pltpu.VMEM((2, TILE, w_width), BF16),
            pltpu.VMEM((rows + 16, LANES), F32),
            pltpu.VMEM((rows, s_width), BF16),
            pltpu.VMEM((rows, w_width), BF16),
            pltpu.VMEM((rows, w_width), BF16),
            pltpu.VMEM((3, LANES, rows), F32),
            pltpu.VMEM((2, rows, s_width), F32),
            pltpu.VMEM((2, rows, s_width), BF16),
            pltpu.VMEM((4, heads, rows), F32),
            pltpu.VMEM((CLIQUE, 8, LANES), F32),
            pltpu.VMEM((8, s_width), F32),
            pltpu.VMEM((2, STATE, s_width), F32),
            pltpu.VMEM((2, STATE, s_width), BF16),
            pltpu.VMEM((STATE, s_width), BF16),
            pltpu.VMEM((STATE, s_width), F32),
            pltpu.VMEM((STATE, s_width), BF16),
            pltpu.VMEM((STATE, s_width), BF16),
            pltpu.VMEM((STATE, s_width), BF16),
            pltpu.VMEM((STATE, s_width), BF16),
            pltpu.VMEM((STATE, s_width), BF16),
            pltpu.VMEM((2, STATE, s_width), BF16),
            pltpu.VMEM((rows, s_width), F32),
            pltpu.VMEM((2, outer, rows, q_width), BF16),
            pltpu.VMEM((CLIQUE,) + final_mapping_matrix.shape, BF16),
            pltpu.VMEM((outer, CLIQUE, rows, width), F32),
            pltpu.VMEM((outer, tps) + block, BF16),
            pltpu.VMEM((outer, tps) + block, BF16),
            pltpu.VMEM((outer,) + block, BF16),
            pltpu.VMEM((outer,) + block, BF16),
            pltpu.SemaphoreType.DMA((2, 2, 5)),
            pltpu.SemaphoreType.DMA((2, CLIQUE)),
            pltpu.SemaphoreType.DMA((2, 3, 2 * PARTS)),
            pltpu.SemaphoreType.DMA((2, 4, CHUNKS)),
            pltpu.SemaphoreType.DMA((2, 2, outer)),
            pltpu.SemaphoreType.DMA((2, 2)),
            pltpu.SemaphoreType.DMA((2, outer, tps)),
            pltpu.SemaphoreType.DMA((2, outer)),
            pltpu.SemaphoreType.DMA,
        ],
        compiler_params=pltpu.CompilerParams(collective_id=1, has_side_effects=True),
    )(
        asking_matrix,
        matching_key_matrix,
        carried_value_matrix,
        silu_switch_argument,
        duality_source_matrix,
        storing_direction_matrix,
        fetching_direction_matrix,
        duality_kernel_coefficients,
        storing_kernel_coefficients,
        fetching_kernel_coefficients,
        raw_increment_lengths,
        logarithmic_fading_speeds,
        token_fading_spikes,
        absorber_score_vector,
        cluster_scaling_factor.reshape(1, s_width),
        final_mapping_matrix,
        cosine,
        sine,
    )


def solution(mesh):
    in_specs = (
        P("sp", "tp"),
        P("sp", "tp"),
        P("sp", "tp"),
        P("sp", "tp"),
        P("sp", "tp"),
        P("sp", "tp"),
        P("sp", "tp"),
        P(None, "tp"),
        P(None, "tp"),
        P(None, "tp"),
        P(None, "tp", "sp"),
        P(None, "tp"),
        P(None, "tp", "sp"),
        P("tp"),
        P("tp"),
        P(None, "tp", "sp"),
    )
    out_specs = P(("sp", "tp"), None)
    return jax.shard_map(local, mesh=mesh, in_specs=in_specs, out_specs=out_specs, check_vma=False)
```

```python
import functools

import jax
import jax.numpy as jnp
import numpy as np
from jax import lax
from jax.experimental import pallas as pl
from jax.experimental.pallas import tpu as pltpu
from jax.sharding import PartitionSpec as P

HEAD = 128
SSD_HEAD = 64
STATE = 128
CONV = 5
WINDOW = 128
CLIQUE = 4
TILE = 8
LANES = 128
CHUNKS = 4
PARTS = 4
SPLIT = 2

ROTARY_BASE = 500000.0
EPSILON = 1e-06

F32 = jnp.float32
BF16 = jnp.bfloat16


def sending(source, target, send_sem, recv_sem, partner):
    return pltpu.make_async_remote_copy(
        src_ref=source,
        dst_ref=target,
        send_sem=send_sem,
        recv_sem=recv_sem,
        device_id=partner,
        device_id_type=pl.DeviceIdType.MESH,
    )


def dot(a, b):
    return jnp.dot(a, b, preferred_element_type=F32)


def dot_t(a, b):
    return lax.dot_general(a, b, (((1,), (1,)), ((), ())), preferred_element_type=F32)


def iota(shape, axis):
    return lax.broadcasted_iota(jnp.int32, shape, axis)


def silu(v):
    return v / (1.0 + jnp.exp(-v))


def split(value):
    high = value.astype(BF16)
    return high, (value - high.astype(F32)).astype(BF16)


def mixer_kernel(
    outer,
    tps,
    q_hbm,
    k_hbm,
    v_hbm,
    gate_hbm,
    src_hbm,
    wr_hbm,
    rd_hbm,
    src_taps_hbm,
    wr_taps_hbm,
    rd_taps_hbm,
    inc_hbm,
    fade_hbm,
    spike_hbm,
    sink_hbm,
    gain_hbm,
    weight_hbm,
    cos_hbm,
    sin_hbm,
    base_hbm,
    out_ref,
    q_ref,
    k_ref,
    v_ref,
    gate_ref,
    src_ref,
    wr_ref,
    rd_ref,
    src_taps,
    wr_taps,
    rd_taps,
    inc_ref,
    fade_ref,
    spike_ref,
    sink_ref,
    gain_ref,
    cos_ref,
    sin_ref,
    base_ref,
    turned,
    k_halo,
    v_halo,
    src_halo,
    wr_halo,
    rd_halo,
    padded,
    xs,
    wv,
    rv,
    square,
    grown,
    scaled,
    rows_log,
    logs,
    decays,
    own_state,
    state_out,
    mate_state,
    total,
    total_out,
    partner_total,
    z_out,
    z_in,
    chip_out,
    incoming,
    y_sum,
    acts,
    weights,
    acc,
    partial,
    pieces,
    summed,
    landed,
    halo_sems,
    log_sems,
    weight_sems,
    scan_sems,
    act_sems,
    own_sems,
    piece_sems,
    out_sems,
    load_sems,
):
    count = outer * CLIQUE
    rows = q_ref.shape[0]
    me = lax.axis_index("sp")
    lane = lax.axis_index("tp")
    spot = lax.rem(me, CLIQUE)
    layer = me // CLIQUE
    base = me - spot
    core = lax.rem(spot, 2)
    side_y = spot // 2
    mate = base + spot + 1 - 2 * core
    partner = base + lax.rem(spot + 2, CLIQUE)
    across = base + CLIQUE - 1 - spot
    way = 1 - core
    step = 1 - 2 * way
    before = layer - step
    after = layer + step
    has_before = (before >= 0) & (before < outer)
    has_after = (after >= 0) & (after < outer)
    later = (side_y + way) == 1
    has_left = me > 0
    has_right = me < count - 1
    left = {"sp": me - 1}
    right = {"sp": me + 1}

    def at_layer(other):
        return {"sp": other * CLIQUE + spot}

    loads = [
        pltpu.make_async_copy(source, target, load_sems.at[index])
        for index, (source, target) in enumerate(
            (
                (base_hbm, base_ref),
                (src_hbm, src_ref),
                (wr_hbm, wr_ref),
                (rd_hbm, rd_ref),
                (k_hbm, k_ref),
                (cos_hbm, cos_ref),
                (sin_hbm, sin_ref),
                (inc_hbm, inc_ref),
                (fade_hbm, fade_ref),
                (spike_hbm, spike_ref),
                (src_taps_hbm, src_taps),
                (wr_taps_hbm, wr_taps),
                (rd_taps_hbm, rd_taps),
                (v_hbm, v_ref),
                (q_hbm, q_ref),
                (sink_hbm, sink_ref),
                (weight_hbm, weights.at[spot]),
                (gate_hbm, gate_ref),
                (gain_hbm, gain_ref),
            )
        )
    ]
    for load in loads:
        load.start()
    barrier = pltpu.get_barrier_semaphore()

    def hail(who):
        pl.semaphore_signal(
            barrier, inc=1, device_id=who, device_id_type=pl.DeviceIdType.MESH
        )

    for other in (mate, partner, across):
        hail({"sp": other})
    for d in range(1, outer):
        hail(at_layer(lax.rem(layer + d, outer)))
    for d in range(1, tps):
        hail({"tp": lax.rem(lane + d, tps)})
    extra_right = (spot == CLIQUE - 1) & has_right
    extra_left = (spot == 0) & has_left
    pl.when(extra_right)(lambda: hail(right))
    pl.when(extra_left)(lambda: hail(left))
    hails = CLIQUE - 1 + outer - 1 + tps - 1

    def loaded(*indices):
        for index in indices:
            loads[index].wait()


    loaded(1, 2, 3)
    pl.semaphore_wait(
        barrier, hails + extra_right.astype(jnp.int32) + extra_left.astype(jnp.int32)
    )

    rims = (
        (src_ref, src_halo, TILE),
        (wr_ref, wr_halo, TILE),
        (rd_ref, rd_halo, TILE),
        (turned, k_halo, rows),
        (v_ref, v_halo, rows),
    )

    def rim_copy(index, to_right):
        source, target, depth = rims[index]
        side = 0 if to_right else 1
        first = rows - depth if to_right else 0
        return sending(
            source.at[first : first + depth, :],
            target.at[side],
            halo_sems.at[0, side, index],
            halo_sems.at[1, side, index],
            right if to_right else left,
        )

    def rims_do(indices, what):
        for index in indices:
            if what == "start":
                pl.when(has_right)(lambda: rim_copy(index, True).start())
                pl.when(has_left)(lambda: rim_copy(index, False).start())
            elif what == "recv":
                pl.when(has_left)(lambda: rim_copy(index, True).wait_recv())
                pl.when(has_right)(lambda: rim_copy(index, False).wait_recv())
            else:
                pl.when(has_right)(lambda: rim_copy(index, True).wait_send())
                pl.when(has_left)(lambda: rim_copy(index, False).wait_send())

    rims_do(range(3), "start")

    def clear(side):
        for _, target, _ in rims:
            target[side] = jnp.zeros(target.shape[1:], target.dtype)

    pl.when(jnp.logical_not(has_left))(lambda: clear(0))
    pl.when(jnp.logical_not(has_right))(lambda: clear(1))

    def clear_in():
        z_in[...] = jnp.zeros_like(z_in)

    pl.when(jnp.logical_not(has_before))(clear_in)

    loaded(0, 4, 5, 6)
    base_cos = base_ref[0, pl.ds(me, 1), :]
    base_sin = base_ref[1, pl.ds(me, 1), :]
    cosine = base_cos * cos_ref[...] - base_sin * sin_ref[...]
    sine = base_sin * cos_ref[...] + base_cos * sin_ref[...]
    sine = jnp.where(iota((rows, HEAD), 1) < HEAD // 2, -sine, sine)

    def turn(block):
        block = block.astype(F32)
        return (block * cosine + pltpu.roll(block, HEAD // 2, 1) * sine).astype(BF16)

    kv_heads = k_ref.shape[1] // HEAD
    for g in range(kv_heads):
        cols = slice(g * HEAD, (g + 1) * HEAD)
        turned[:, cols] = turn(k_ref[:, cols])

    loaded(7, 8, 9)
    heads = inc_ref.shape[1]
    gap = LANES // 4
    lane_at = iota((heads, rows), 1)
    eye = iota((heads, heads), 0) == iota((heads, heads), 1)
    steps = []
    runs = []
    for d in range(2):
        raw = inc_ref[d]
        length = jnp.maximum(raw, 0.0) + jnp.log1p(jnp.exp(-jnp.abs(raw)))
        rate = jnp.sum(
            jnp.where(eye, jnp.broadcast_to(jnp.exp(fade_ref[d : d + 1, :]), (heads, heads)), 0.0),
            axis=1,
            keepdims=True,
        )
        run = spike_ref[d] - rate * length
        hop = 1
        while hop < rows:
            if d == 0:
                moved = jnp.where(lane_at >= hop, pltpu.roll(run, hop, 1), 0.0)
            else:
                moved = jnp.where(lane_at < rows - hop, pltpu.roll(run, rows - hop, 1), 0.0)
            run = run + moved
            hop *= 2
        steps.append(length)
        runs.append(run)
    ends = [runs[0][:, rows - 1 : rows], runs[1][:, 0:1]]
    square[...] = jnp.zeros_like(square)
    for d in range(2):
        square[0, d * gap : d * gap + heads, :] = runs[d]
        fill = jnp.exp(runs[d])
        high = fill.astype(BF16).astype(F32)
        square[1, 2 * d * gap : 2 * d * gap + heads, :] = high
        square[1, (2 * d + 1) * gap : (2 * d + 1) * gap + heads, :] = fill - high
        fill = steps[d] * jnp.exp(ends[d] - runs[d])
        high = fill.astype(BF16).astype(F32)
        square[2, 2 * d * gap : 2 * d * gap + heads, :] = high
        square[2, (2 * d + 1) * gap : (2 * d + 1) * gap + heads, :] = fill - high
        rows_log[d] = runs[d]
        rows_log[2 + d] = steps[d]
    run_cols = square[0].T
    log_row = iota((8, LANES), 0)
    logs[spot] = jnp.where(
        log_row == 0,
        jnp.broadcast_to(run_cols[rows - 1 : rows, :], (8, LANES)),
        jnp.broadcast_to(run_cols[0:1, :], (8, LANES)),
    )

    def log_copy(flip, who, slot):
        return sending(
            logs.at[slot],
            logs.at[slot],
            log_sems.at[0, flip],
            log_sems.at[1, flip],
            {"sp": base + who},
        )

    flips = (
        spot + 1 - 2 * core,
        lax.rem(spot + 2, CLIQUE),
        CLIQUE - 1 - spot,
    )
    for flip, who in enumerate(flips):
        log_copy(flip, who, spot).start()

    loaded(13)
    rims_do(range(3, 5), "start")

    loaded(16)

    def weight_part(slot, index):
        return weights.at[slot, index]

    def weight_mate(slot):
        return sending(
            weights.at[slot],
            weights.at[slot],
            weight_sems.at[0, 0, 0],
            weight_sems.at[1, 0, 0],
            {"sp": mate},
        )

    def weight_over(index, slot):
        return sending(
            weight_part(slot, index),
            weight_part(slot, index),
            weight_sems.at[0, 1, index],
            weight_sems.at[1, 1, index],
            {"sp": partner},
        )

    def weight_onward(index, slot):
        return sending(
            weight_part(slot, index),
            weight_part(slot, index),
            weight_sems.at[0, 2, index],
            weight_sems.at[1, 2, index],
            {"sp": mate},
        )

    def pass_on(index):
        weight_over(index, flips[1]).wait_recv()
        weight_onward(index, flips[1]).start()


    loaded(10, 11, 12)
    rims_do(range(3), "recv")
    columns = ((src_ref, src_halo, src_taps, xs), (wr_ref, wr_halo, wr_taps, wv), (rd_ref, rd_halo, rd_taps, rv))
    margin = CONV // 2
    for source, halo, taps_ref, target in columns:
        width = source.shape[1]
        taps = taps_ref[...].astype(F32)
        for first in range(0, width, LANES):
            cols = slice(first, first + LANES)
            padded[8 : 8 + rows, :] = source[:, cols].astype(F32)
            padded[0:8, :] = halo[0, :, cols].astype(F32)
            padded[8 + rows : 16 + rows, :] = halo[1, :, cols].astype(F32)
            value = jnp.zeros((rows, LANES), F32)
            for k in range(CONV):
                start = 8 - margin + k
                value = value + padded[start : start + rows, :] * taps[k : k + 1, cols]
            target[:, cols] = silu(value).astype(BF16)

    def own_copy(half, way_up):
        target = layer + (1 if way_up else -1)
        return sending(
            acts.at[half, layer],
            acts.at[half, layer],
            own_sems.at[half, 1 if way_up else 0],
            act_sems.at[1, half, layer],
            at_layer(target),
        )

    part_wide = acts.shape[3]

    def put(half, cols, value):
        first = cols.start
        while first < cols.stop:
            part = first // part_wide
            last = min(cols.stop, (part + 1) * part_wide)
            acts[2 * half + part, layer, :, first - part * part_wide : last - part * part_wide] = value[
                :, first - cols.start : last - cols.start
            ].astype(BF16)
            first = last

    can_up = layer < outer - 1
    can_down = layer > 0

    def own_start(half):
        pl.when(can_up)(lambda: own_copy(half, True).start())
        pl.when(can_down)(lambda: own_copy(half, False).start())

    def far_copy(half, block, sign):
        return sending(
            acts.at[half, block],
            acts.at[half, block],
            act_sems.at[0, half, block],
            act_sems.at[1, half, block],
            at_layer(layer - sign),
        )

    def each(d, do):
        for sign in (-1, 1):
            block = layer + sign * d
            pl.when((block >= 0) & (block < outer))(functools.partial(do, block, sign))

    def relay(half, d):
        def do(block, sign):
            copy = far_copy(half, block, sign)
            copy.wait_recv()
            target = layer - sign
            pl.when((target >= 0) & (target < outer))(lambda: copy.start())

        each(d, do)

    groups = wr_ref.shape[1] // STATE
    wide = xs.shape[1]
    group_wide = wide // groups
    per_group = group_wide // SSD_HEAD
    owner = iota((LANES, wide), 1) // SSD_HEAD
    place = iota((LANES, wide), 0)
    pick = []
    for d in range(2):
        hit = (place == owner + 2 * d * gap) | (place == owner + (2 * d + 1) * gap)
        pick.append(jnp.where(hit, 1.0, 0.0).astype(BF16))
    grow_cols = square[1].T.astype(BF16)
    scale_cols = square[2].T.astype(BF16)
    for d in range(2):
        grown[d] = dot(grow_cols, pick[d])
        scaled[d] = (dot(scale_cols, pick[d]) * xs[...].astype(F32)).astype(BF16)
    for g in range(groups):
        cols = slice(g * group_wide, (g + 1) * group_wide)
        write_t = wv[:, g * STATE : (g + 1) * STATE].astype(F32).T.astype(BF16)
        for d in range(2):
            fresh = dot(write_t, scaled[d, :, cols])
            own_state[d, :, cols] = fresh
            state_out[d, :, cols] = fresh.astype(BF16)

    swap = sending(
        state_out.at[1 - way],
        mate_state,
        scan_sems.at[0, 0, 0],
        scan_sems.at[1, 0, 0],
        {"sp": mate},
    )
    swap.start()
    weight_mate(spot).start()

    for flip, who in enumerate(flips):
        log_copy(flip, who, who).wait_recv()
    log_own = logs[spot, pl.ds(way, 1), :]
    log_mate = logs[flips[0], pl.ds(way, 1), :]
    log_partner = logs[flips[1], pl.ds(way, 1), :] + logs[flips[2], pl.ds(way, 1), :]
    log_rows = jnp.where(
        log_row == 0,
        jnp.broadcast_to(log_own, (8, LANES)),
        jnp.where(
            log_row == 1,
            jnp.broadcast_to(log_mate, (8, LANES)),
            jnp.where(
                log_row == 2,
                jnp.broadcast_to(log_partner, (8, LANES)),
                jnp.broadcast_to(log_own + log_mate, (8, LANES)),
            ),
        ),
    )
    high, low = split(jnp.exp(log_rows))
    mine = jnp.where(place == owner + way * gap, 1.0, 0.0).astype(BF16)
    decays[...] = dot(high, mine) + dot(low, mine)
    dec_own = decays[0:1, :]
    dec_mate = decays[1:2, :]
    dec_partner = decays[2:3, :]
    dec_chip = decays[3:4, :]
    dec_layer = dec_partner * dec_chip
    one = jnp.ones_like(dec_own)
    from_partner = jnp.where(later, dec_chip, one)
    from_mine = jnp.where(later, one, dec_partner)
    in_before = jnp.where(later, dec_partner, one)
    in_partner = jnp.where(later, 1.0, 0.0)

    chunk = STATE // CHUNKS

    def over_copy(c):
        part = slice(c * chunk, (c + 1) * chunk)
        return sending(
            total_out.at[part, :],
            partner_total.at[part, :],
            scan_sems.at[0, 1, c],
            scan_sems.at[1, 1, c],
            {"sp": partner},
        )

    def z_copy(c, to):
        part = slice(c * chunk, (c + 1) * chunk)
        return sending(
            z_out.at[part, :],
            z_in.at[part, :],
            scan_sems.at[0, 2, c],
            scan_sems.at[1, 2, c],
            at_layer(to),
        )

    def down_copy(c):
        part = slice(c * chunk, (c + 1) * chunk)
        return sending(
            chip_out.at[part, :],
            incoming.at[way, part, :],
            scan_sems.at[0, 3, c],
            scan_sems.at[1, 3, c],
            {"sp": mate},
        )

    def down_recv(c):
        part = slice(c * chunk, (c + 1) * chunk)
        return sending(
            chip_out.at[part, :],
            incoming.at[1 - way, part, :],
            scan_sems.at[0, 3, c],
            scan_sems.at[1, 3, c],
            {"sp": mate},
        )

    run_at = square[0].T
    causal = iota((rows, rows), 1) <= iota((rows, rows), 0)
    diagonal = iota((rows, rows), 1) == iota((rows, rows), 0)

    def within(g):
        read = rv[:, g * STATE : (g + 1) * STATE]
        write = wv[:, g * STATE : (g + 1) * STATE]
        affinity = dot_t(read, write)
        for j in range(per_group):
            h = g * per_group + j
            cols = slice(h * SSD_HEAD, (h + 1) * SSD_HEAD)
            ahead = run_at[:, h : h + 1] - rows_log[0, h : h + 1, :]
            back = run_at[:, gap + h : gap + h + 1] - rows_log[1, h : h + 1, :]
            fade = jnp.exp(jnp.where(causal, ahead, back))
            length_f = rows_log[2, h : h + 1, :]
            length_b = rows_log[3, h : h + 1, :]
            taken = jnp.where(causal, length_f, length_b) * fade
            taken = taken + jnp.where(diagonal, length_b, 0.0)
            y_sum[:, cols] = dot((affinity * taken).astype(BF16), xs[:, cols])

    for g in range(groups):
        within(g)
    swap.wait_recv()
    for c in range(CHUNKS):
        part = slice(c * chunk, (c + 1) * chunk)
        summed_state = (
            mate_state[part, :].astype(F32) * dec_own + own_state[way, part, :]
        )
        total[part, :] = summed_state
        total_out[part, :] = summed_state.astype(BF16)
        over_copy(c).start()

    rims_do(range(3, 5), "recv")
    loaded(14, 15)
    sharing = q_ref.shape[1] // HEAD // kv_heads
    stacked = (sharing * rows, rows)
    query_at = lax.rem(iota(stacked, 0), rows)
    above = iota(stacked, 1) >= query_at
    below = iota(stacked, 1) <= query_at
    ok_left = above & has_left
    ok_right = below & has_right
    scale = HEAD ** (-0.5)
    for g in range(kv_heads):
        cols = slice(g * HEAD, (g + 1) * HEAD)
        keys = (k_halo[0, :, cols], turned[:, cols], k_halo[1, :, cols])
        values = (v_halo[0, :, cols], v_ref[:, cols], v_halo[1, :, cols])
        first = g * sharing
        query = jnp.concatenate(
            [turn(q_ref[:, h * HEAD : (h + 1) * HEAD]) for h in range(first, first + sharing)], axis=0
        )
        tiles = [dot_t(query, key) * scale for key in keys]
        tiles[0] = jnp.where(ok_left, tiles[0], -jnp.inf)
        tiles[2] = jnp.where(ok_right, tiles[2], -jnp.inf)
        sink = jnp.concatenate(
            [jnp.broadcast_to(sink_ref[:, h : h + 1], (rows, 1)) for h in range(first, first + sharing)],
            axis=0,
        )
        top = jnp.maximum(
            jnp.max(jnp.maximum(jnp.maximum(tiles[0], tiles[1]), tiles[2]), axis=1, keepdims=True),
            sink,
        )
        tiles = [jnp.exp(tile - top) for tile in tiles]
        bottom = jnp.sum(tiles[0] + tiles[1] + tiles[2], axis=1, keepdims=True) + jnp.exp(sink - top)
        inverse = 1.0 / bottom
        found = jnp.zeros((sharing * rows, HEAD), F32)
        for tile, value in zip(tiles, values):
            found = found + dot((tile * inverse).astype(BF16), value)
        for j in range(sharing):
            h = first + j
            put(0, slice(h * HEAD, (h + 1) * HEAD), found[j * rows : (j + 1) * rows])
    own_start(0)
    own_start(1)

    for c in range(CHUNKS):
        part = slice(c * chunk, (c + 1) * chunk)
        over_copy(c).wait_recv()
        level = partner_total[part, :].astype(F32) * from_partner + total[part, :] * from_mine
        total[part, :] = level

        def first_out():
            z_out[part, :] = level.astype(BF16)
            z_copy(c, after).start()

        pl.when(jnp.logical_not(has_before) & has_after)(first_out)
    for index in range(PARTS):
        weight_over(index, spot).start()
    if outer > 1:
        relay(0, 1)
        relay(1, 1)
    for c in range(CHUNKS):
        part = slice(c * chunk, (c + 1) * chunk)

        def next_out():
            z_copy(c, after).wait_recv()

            def send():
                z_out[part, :] = (
                    z_in[part, :].astype(F32) * dec_layer + total[part, :]
                ).astype(BF16)
                z_copy(c, after).start()

            pl.when(has_after)(send)

        pl.when(has_before)(next_out)
        entering = z_in[part, :].astype(F32)
        chip_in = entering * in_before + partner_total[part, :].astype(F32) * in_partner
        chip_out[part, :] = chip_in.astype(BF16)
        down_copy(c).start()
        incoming[way, part, :] = (
            chip_in * dec_mate + mate_state[part, :].astype(F32)
        ).astype(BF16)
    for d in range(2, outer):
        relay(0, d)
        relay(1, d)
        if d == 2:
            break
    for c in range(CHUNKS):
        down_recv(c).wait_recv()

    loaded(17, 18)
    for g in range(groups):
        cols = slice(g * group_wide, (g + 1) * group_wide)
        read = rv[:, g * STATE : (g + 1) * STATE]
        value = y_sum[:, cols]
        for d in range(2):
            value = value + dot(read, incoming[d, :, cols]) * grown[d, :, cols]
        value = value * silu(gate_ref[:, cols].astype(F32))
        mean = jnp.sum(value * value, axis=1, keepdims=True) * (1.0 / group_wide)
        value = value * lax.rsqrt(mean + EPSILON) * gain_ref[:, cols]
        put(1, cols, value)
    own_start(2)
    own_start(3)

    share = rows // tps

    def multiply_first(block, sign):
        def body(slot, carry):
            acc[block, slot] = dot(acts[0, block], weights[slot, 0]) + dot(
                acts[1, block], weights[slot, 1]
            )
            return carry

        lax.fori_loop(0, CLIQUE, body, 0)

    def piece_copy(block, part, other, slot):
        span = pl.ds(part * SPLIT, SPLIT)
        return sending(
            partial.at[block, other, span],
            pieces.at[block, slot, span],
            piece_sems.at[0, block, other, part],
            piece_sems.at[1, block, slot, part],
            {"tp": other},
        )

    lanes = [lax.rem(lane + d, tps) for d in range(1, tps)]

    def multiply_third(block, sign):
        def body(slot, carry):
            acc[block, slot] += dot(acts[2, block], weights[slot, 2])
            return carry

        lax.fori_loop(0, CLIQUE, body, 0)

    def multiply_second(block, sign):
        def body(slot, carry):
            product = (acc[block, slot] + dot(acts[3, block], weights[slot, 3])).astype(BF16)
            for other in range(tps):
                partial[block, other, slot] = product[other * share : (other + 1) * share]
            return carry

        for part in range(CLIQUE // SPLIT):
            lax.fori_loop(part * SPLIT, (part + 1) * SPLIT, body, 0)
            for other in lanes:
                piece_copy(block, part, other, lane).start()

    def out_copy(block, slot, part):
        span = pl.ds(part * SPLIT, SPLIT)
        return sending(
            summed.at[block, span],
            landed.at[slot, span],
            out_sems.at[0, block, part],
            out_sems.at[1, slot, part],
            at_layer(block),
        )

    def settle(block, sign):
        for part in range(CLIQUE // SPLIT):
            span = slice(part * SPLIT, (part + 1) * SPLIT)
            result = partial[block, lane, span].astype(F32)
            for other in lanes:
                piece_copy(block, part, other, other).wait_recv()
                result = result + pieces[block, other, span].astype(F32)
            if sign:
                summed[block, span] = result.astype(BF16)
                out_copy(block, layer, part).start()
            else:
                landed[layer, span] = result.astype(BF16)

    weight_mate(flips[0]).wait_recv()
    for index in range(2):
        pass_on(index)
    for index in range(2):
        weight_onward(index, flips[2]).wait_recv()
    multiply_first(layer, 0)
    if outer > 1:
        each(1, multiply_first)
    if outer > 1:
        relay(2, 1)
        relay(3, 1)
    for d in range(2, outer):
        if d > 2:
            relay(0, d)
            relay(1, d)
        each(d, multiply_first)
    for index in range(2, PARTS):
        pass_on(index)
    for index in range(2, PARTS):
        weight_onward(index, flips[2]).wait_recv()
    multiply_third(layer, 0)
    multiply_second(layer, 0)
    if outer > 1:
        each(1, multiply_third)
        each(1, multiply_second)
    for d in range(2, outer):
        relay(2, d)
        each(d, multiply_third)
        relay(3, d)
        each(d, multiply_second)
        if d == 2:
            settle(layer, 0)
        each(d - 1, settle)
    if outer < 3:
        settle(layer, 0)
    if outer > 1:
        each(outer - 1, settle)

    def arrive(block, sign):
        for part in range(CLIQUE // SPLIT):
            out_copy(block, block, part).wait_recv()

    for d in range(1, outer):
        each(d, arrive)
    width = landed.shape[3]
    for other in range(outer):
        for slot in range(CLIQUE):
            first = (other * CLIQUE + slot) * width
            out_ref[:, first : first + width] = landed[other, slot]

    rims_do(range(5), "send")
    for flip, who in enumerate(flips):
        log_copy(flip, who, spot).wait_send()
    weight_mate(spot).wait_send()
    for half in range(PARTS):
        pl.when(can_up)(lambda: own_copy(half, True).wait_send())
        pl.when(can_down)(lambda: own_copy(half, False).wait_send())
    for index in range(PARTS):
        weight_over(index, spot).wait_send()
        weight_onward(index, flips[1]).wait_send()
    swap.wait_send()
    for c in range(CHUNKS):
        over_copy(c).wait_send()
        down_copy(c).wait_send()
        pl.when(has_after)(lambda: z_copy(c, after).wait_send())

    def gone(block, sign):
        target = layer - sign
        for half in range(PARTS):
            pl.when((target >= 0) & (target < outer))(
                lambda: far_copy(half, block, sign).wait_send()
            )
        for part in range(CLIQUE // SPLIT):
            out_copy(block, layer, part).wait_send()
            for other in lanes:
                piece_copy(block, part, other, lane).wait_send()

    for d in range(1, outer):
        each(d, gone)
    for part in range(CLIQUE // SPLIT):
        for other in lanes:
            piece_copy(layer, part, other, lane).wait_send()


def local(
    asking_matrix,
    matching_key_matrix,
    carried_value_matrix,
    silu_switch_argument,
    duality_source_matrix,
    storing_direction_matrix,
    fetching_direction_matrix,
    duality_kernel_coefficients,
    storing_kernel_coefficients,
    fetching_kernel_coefficients,
    raw_increment_lengths,
    logarithmic_fading_speeds,
    token_fading_spikes,
    absorber_score_vector,
    cluster_scaling_factor,
    final_mapping_matrix,
):
    count = lax.axis_size("sp")
    tps = lax.axis_size("tp")
    outer = count // CLIQUE
    rows, q_width = asking_matrix.shape
    k_width = matching_key_matrix.shape[1]
    s_width = duality_source_matrix.shape[1]
    w_width = storing_direction_matrix.shape[1]
    heads = raw_increment_lengths.shape[1]
    width = final_mapping_matrix.shape[2]
    share = rows // tps
    halfway = HEAD // 2
    spacing = ROTARY_BASE ** (-np.arange(halfway, dtype=np.float64) * 2.0 / HEAD)
    spacing = np.concatenate([spacing, spacing])
    angles = np.arange(rows, dtype=np.float64)[:, None] * spacing[None, :]
    firsts = np.arange(count, dtype=np.float64)[:, None] * rows * spacing[None, :]
    turns = np.stack([np.cos(firsts), np.sin(firsts)]).astype(np.float32)
    block = (CLIQUE, share, width)
    return pl.pallas_call(
        functools.partial(mixer_kernel, outer, tps),
        out_shape=jax.ShapeDtypeStruct((share, count * width), BF16),
        in_specs=[pl.BlockSpec(memory_space=pl.ANY)] * 19,
        out_specs=pl.BlockSpec(memory_space=pltpu.VMEM),
        scratch_shapes=[
            pltpu.VMEM((rows, q_width), BF16),
            pltpu.VMEM((rows, k_width), BF16),
            pltpu.VMEM((rows, k_width), BF16),
            pltpu.VMEM((rows, s_width), BF16),
            pltpu.VMEM((rows, s_width), BF16),
            pltpu.VMEM((rows, w_width), BF16),
            pltpu.VMEM((rows, w_width), BF16),
            pltpu.VMEM((CONV, s_width), BF16),
            pltpu.VMEM((CONV, w_width), BF16),
            pltpu.VMEM((CONV, w_width), BF16),
            pltpu.VMEM((2, heads, rows), F32),
            pltpu.VMEM((2, heads), F32),
            pltpu.VMEM((2, heads, rows), F32),
            pltpu.VMEM((1, q_width // HEAD), F32),
            pltpu.VMEM((1, s_width), F32),
            pltpu.VMEM((rows, HEAD), F32),
            pltpu.VMEM((rows, HEAD), F32),
            pltpu.VMEM((2, count, HEAD), F32),
            pltpu.VMEM((rows, k_width), BF16),
            pltpu.VMEM((2, rows, k_width), BF16),
            pltpu.VMEM((2, rows, k_width), BF16),
            pltpu.VMEM((2, TILE, s_width), BF16),
            pltpu.VMEM((2, TILE, w_width), BF16),
            pltpu.VMEM((2, TILE, w_width), BF16),
            pltpu.VMEM((rows + 16, LANES), F32),
            pltpu.VMEM((rows, s_width), BF16),
            pltpu.VMEM((rows, w_width), BF16),
            pltpu.VMEM((rows, w_width), BF16),
            pltpu.VMEM((3, LANES, rows), F32),
            pltpu.VMEM((2, rows, s_width), F32),
            pltpu.VMEM((2, rows, s_width), BF16),
            pltpu.VMEM((4, heads, rows), F32),
            pltpu.VMEM((CLIQUE, 8, LANES), F32),
            pltpu.VMEM((8, s_width), F32),
            pltpu.VMEM((2, STATE, s_width), F32),
            pltpu.VMEM((2, STATE, s_width), BF16),
            pltpu.VMEM((STATE, s_width), BF16),
            pltpu.VMEM((STATE, s_width), F32),
            pltpu.VMEM((STATE, s_width), BF16),
            pltpu.VMEM((STATE, s_width), BF16),
            pltpu.VMEM((STATE, s_width), BF16),
            pltpu.VMEM((STATE, s_width), BF16),
            pltpu.VMEM((STATE, s_width), BF16),
            pltpu.VMEM((2, STATE, s_width), BF16),
            pltpu.VMEM((rows, s_width), F32),
            pltpu.VMEM((PARTS, outer, rows, q_width // 2), BF16),
            pltpu.VMEM((CLIQUE, PARTS, q_width // 2, width), BF16),
            pltpu.VMEM((outer, CLIQUE, rows, width), F32),
            pltpu.VMEM((outer, tps) + block, BF16),
            pltpu.VMEM((outer, tps) + block, BF16),
            pltpu.VMEM((outer,) + block, BF16),
            pltpu.VMEM((outer,) + block, BF16),
            pltpu.SemaphoreType.DMA((2, 2, 5)),
            pltpu.SemaphoreType.DMA((2, CLIQUE)),
            pltpu.SemaphoreType.DMA((2, 3, PARTS)),
            pltpu.SemaphoreType.DMA((2, 4, CHUNKS)),
            pltpu.SemaphoreType.DMA((2, PARTS, outer)),
            pltpu.SemaphoreType.DMA((PARTS, 2)),
            pltpu.SemaphoreType.DMA((2, outer, tps, CLIQUE // SPLIT)),
            pltpu.SemaphoreType.DMA((2, outer, CLIQUE // SPLIT)),
            pltpu.SemaphoreType.DMA((19,)),
        ],
        compiler_params=pltpu.CompilerParams(collective_id=1, has_side_effects=True),
    )(
        asking_matrix,
        matching_key_matrix,
        carried_value_matrix,
        silu_switch_argument,
        duality_source_matrix,
        storing_direction_matrix,
        fetching_direction_matrix,
        duality_kernel_coefficients,
        storing_kernel_coefficients,
        fetching_kernel_coefficients,
        raw_increment_lengths,
        logarithmic_fading_speeds,
        token_fading_spikes,
        absorber_score_vector.reshape(1, q_width // HEAD),
        cluster_scaling_factor.reshape(1, s_width),
        final_mapping_matrix.reshape(PARTS, q_width // 2, width),
        np.cos(angles).astype(np.float32),
        np.sin(angles).astype(np.float32),
        turns,
    )


def solution(mesh):
    in_specs = (
        P("sp", "tp"),
        P("sp", "tp"),
        P("sp", "tp"),
        P("sp", "tp"),
        P("sp", "tp"),
        P("sp", "tp"),
        P("sp", "tp"),
        P(None, "tp"),
        P(None, "tp"),
        P(None, "tp"),
        P(None, "tp", "sp"),
        P(None, "tp"),
        P(None, "tp", "sp"),
        P("tp"),
        P("tp"),
        P(None, "tp", "sp"),
    )
    out_specs = P(("sp", "tp"), None)
    return jax.shard_map(local, mesh=mesh, in_specs=in_specs, out_specs=out_specs, check_vma=False)
```

```python
import functools

import jax
import jax.numpy as jnp
import numpy as np
from jax import lax
from jax.experimental import pallas as pl
from jax.experimental.pallas import tpu as pltpu
from jax.sharding import PartitionSpec as P

HEAD = 128
SSD_HEAD = 64
STATE = 128
CONV = 5
WINDOW = 128
CLIQUE = 4
TILE = 8
LANES = 128
CHUNKS = 4
PARTS = 4
SPLIT = 2

ROTARY_BASE = 500000.0
EPSILON = 1e-06

F32 = jnp.float32
BF16 = jnp.bfloat16


def sending(source, target, send_sem, recv_sem, partner):
    return pltpu.make_async_remote_copy(
        src_ref=source,
        dst_ref=target,
        send_sem=send_sem,
        recv_sem=recv_sem,
        device_id=partner,
        device_id_type=pl.DeviceIdType.MESH,
    )


def dot(a, b):
    return jnp.dot(a, b, preferred_element_type=F32)


def dot_t(a, b):
    return lax.dot_general(a, b, (((1,), (1,)), ((), ())), preferred_element_type=F32)


def iota(shape, axis):
    return lax.broadcasted_iota(jnp.int32, shape, axis)


def silu(v):
    return v / (1.0 + jnp.exp(-v))


def split(value):
    high = value.astype(BF16)
    return high, (value - high.astype(F32)).astype(BF16)


def mixer_kernel(
    outer,
    tps,
    q_hbm,
    k_hbm,
    v_hbm,
    gate_hbm,
    src_hbm,
    wr_hbm,
    rd_hbm,
    src_taps_hbm,
    wr_taps_hbm,
    rd_taps_hbm,
    inc_hbm,
    fade_hbm,
    spike_hbm,
    sink_hbm,
    gain_hbm,
    weight_hbm,
    cos_hbm,
    sin_hbm,
    base_hbm,
    out_ref,
    q_ref,
    k_ref,
    v_ref,
    gate_ref,
    src_ref,
    wr_ref,
    rd_ref,
    src_taps,
    wr_taps,
    rd_taps,
    inc_ref,
    fade_ref,
    spike_ref,
    sink_ref,
    gain_ref,
    cos_ref,
    sin_ref,
    base_ref,
    turned,
    k_halo,
    v_halo,
    src_halo,
    wr_halo,
    rd_halo,
    padded,
    xs,
    wv,
    rv,
    square,
    grown,
    scaled,
    rows_log,
    logs,
    decays,
    own_state,
    state_out,
    mate_state,
    total,
    total_out,
    partner_total,
    z_out,
    z_in,
    chip_out,
    incoming,
    y_sum,
    acts,
    weights,
    acc,
    partial,
    pieces,
    summed,
    landed,
    spare,
    first_out_sum,
    first_in_sum,
    halo_sems,
    log_sems,
    weight_sems,
    scan_sems,
    act_sems,
    own_sems,
    piece_sems,
    out_sems,
    spare_sems,
    first_sems,
    load_sems,
):
    count = outer * CLIQUE
    rows = q_ref.shape[0]
    me = lax.axis_index("sp")
    lane = lax.axis_index("tp")
    spot = lax.rem(me, CLIQUE)
    layer = me // CLIQUE
    base = me - spot
    core = lax.rem(spot, 2)
    side_y = spot // 2
    mate = base + spot + 1 - 2 * core
    partner = base + lax.rem(spot + 2, CLIQUE)
    across = base + CLIQUE - 1 - spot
    way = 1 - core
    step = 1 - 2 * way
    before = layer - step
    after = layer + step
    has_before = (before >= 0) & (before < outer)
    has_after = (after >= 0) & (after < outer)
    later = (side_y + way) == 1
    has_left = me > 0
    has_right = me < count - 1
    left = {"sp": me - 1}
    right = {"sp": me + 1}

    lean = outer >= 4
    low = (layer < 2).astype(jnp.int32)
    buddy = low * (1 - layer) + (1 - low) * (2 * outer - 3 - layer)
    giver = (layer == 0) | (layer == outer - 1)
    taker = (layer == 1) | (layer == outer - 2)

    def if_giver(do):
        if lean:
            pl.when(giver)(do)

    def if_taker(do):
        if lean:
            pl.when(taker)(do)

    def if_not_giver(do):
        if lean:
            pl.when(jnp.logical_not(giver))(do)
        else:
            do()

    def at_layer(other):
        return {"sp": other * CLIQUE + spot}

    loads = [
        pltpu.make_async_copy(source, target, load_sems.at[index])
        for index, (source, target) in enumerate(
            (
                (base_hbm, base_ref),
                (src_hbm, src_ref),
                (wr_hbm, wr_ref),
                (rd_hbm, rd_ref),
                (k_hbm, k_ref),
                (cos_hbm, cos_ref),
                (sin_hbm, sin_ref),
                (inc_hbm, inc_ref),
                (fade_hbm, fade_ref),
                (spike_hbm, spike_ref),
                (src_taps_hbm, src_taps),
                (wr_taps_hbm, wr_taps),
                (rd_taps_hbm, rd_taps),
                (v_hbm, v_ref),
                (q_hbm, q_ref),
                (sink_hbm, sink_ref),
                (weight_hbm, weights.at[spot]),
                (gate_hbm, gate_ref),
                (gain_hbm, gain_ref),
            )
        )
    ]
    for load in loads:
        load.start()
    barrier = pltpu.get_barrier_semaphore()

    def hail(who):
        pl.semaphore_signal(
            barrier, inc=1, device_id=who, device_id_type=pl.DeviceIdType.MESH
        )

    for other in (mate, partner, across):
        hail({"sp": other})
    for d in range(1, outer):
        hail(at_layer(lax.rem(layer + d, outer)))
    for d in range(1, tps):
        hail({"tp": lax.rem(lane + d, tps)})
    extra_right = (spot == CLIQUE - 1) & has_right
    extra_left = (spot == 0) & has_left
    pl.when(extra_right)(lambda: hail(right))
    pl.when(extra_left)(lambda: hail(left))
    hails = CLIQUE - 1 + outer - 1 + tps - 1

    def loaded(*indices):
        for index in indices:
            loads[index].wait()


    loaded(1, 2, 3)
    pl.semaphore_wait(
        barrier, hails + extra_right.astype(jnp.int32) + extra_left.astype(jnp.int32)
    )

    rims = (
        (src_ref, src_halo, TILE),
        (wr_ref, wr_halo, TILE),
        (rd_ref, rd_halo, TILE),
        (turned, k_halo, rows),
        (v_ref, v_halo, rows),
    )

    def rim_copy(index, to_right):
        source, target, depth = rims[index]
        side = 0 if to_right else 1
        first = rows - depth if to_right else 0
        return sending(
            source.at[first : first + depth, :],
            target.at[side],
            halo_sems.at[0, side, index],
            halo_sems.at[1, side, index],
            right if to_right else left,
        )

    def rims_do(indices, what):
        for index in indices:
            if what == "start":
                pl.when(has_right)(lambda: rim_copy(index, True).start())
                pl.when(has_left)(lambda: rim_copy(index, False).start())
            elif what == "recv":
                pl.when(has_left)(lambda: rim_copy(index, True).wait_recv())
                pl.when(has_right)(lambda: rim_copy(index, False).wait_recv())
            else:
                pl.when(has_right)(lambda: rim_copy(index, True).wait_send())
                pl.when(has_left)(lambda: rim_copy(index, False).wait_send())

    rims_do(range(3), "start")

    def clear(side):
        for _, target, _ in rims:
            target[side] = jnp.zeros(target.shape[1:], target.dtype)

    pl.when(jnp.logical_not(has_left))(lambda: clear(0))
    pl.when(jnp.logical_not(has_right))(lambda: clear(1))

    def clear_in():
        z_in[...] = jnp.zeros_like(z_in)

    pl.when(jnp.logical_not(has_before))(clear_in)

    loaded(0, 4, 5, 6)
    base_cos = base_ref[0, pl.ds(me, 1), :]
    base_sin = base_ref[1, pl.ds(me, 1), :]
    cosine = base_cos * cos_ref[...] - base_sin * sin_ref[...]
    sine = base_sin * cos_ref[...] + base_cos * sin_ref[...]
    sine = jnp.where(iota((rows, HEAD), 1) < HEAD // 2, -sine, sine)

    def turn(block):
        block = block.astype(F32)
        return (block * cosine + pltpu.roll(block, HEAD // 2, 1) * sine).astype(BF16)

    kv_heads = k_ref.shape[1] // HEAD
    for g in range(kv_heads):
        cols = slice(g * HEAD, (g + 1) * HEAD)
        turned[:, cols] = turn(k_ref[:, cols])

    loaded(7, 8, 9)
    heads = inc_ref.shape[1]
    gap = LANES // 4
    lane_at = iota((heads, rows), 1)
    eye = iota((heads, heads), 0) == iota((heads, heads), 1)
    steps = []
    runs = []
    for d in range(2):
        raw = inc_ref[d]
        length = jnp.maximum(raw, 0.0) + jnp.log1p(jnp.exp(-jnp.abs(raw)))
        rate = jnp.sum(
            jnp.where(eye, jnp.broadcast_to(jnp.exp(fade_ref[d : d + 1, :]), (heads, heads)), 0.0),
            axis=1,
            keepdims=True,
        )
        run = spike_ref[d] - rate * length
        hop = 1
        while hop < rows:
            if d == 0:
                moved = jnp.where(lane_at >= hop, pltpu.roll(run, hop, 1), 0.0)
            else:
                moved = jnp.where(lane_at < rows - hop, pltpu.roll(run, rows - hop, 1), 0.0)
            run = run + moved
            hop *= 2
        steps.append(length)
        runs.append(run)
    ends = [runs[0][:, rows - 1 : rows], runs[1][:, 0:1]]
    square[...] = jnp.zeros_like(square)
    for d in range(2):
        square[0, d * gap : d * gap + heads, :] = runs[d]
        fill = jnp.exp(runs[d])
        high = fill.astype(BF16).astype(F32)
        square[1, 2 * d * gap : 2 * d * gap + heads, :] = high
        square[1, (2 * d + 1) * gap : (2 * d + 1) * gap + heads, :] = fill - high
        fill = steps[d] * jnp.exp(ends[d] - runs[d])
        high = fill.astype(BF16).astype(F32)
        square[2, 2 * d * gap : 2 * d * gap + heads, :] = high
        square[2, (2 * d + 1) * gap : (2 * d + 1) * gap + heads, :] = fill - high
        rows_log[d] = runs[d]
        rows_log[2 + d] = steps[d]
    run_cols = square[0].T
    log_row = iota((8, LANES), 0)
    logs[spot] = jnp.where(
        log_row == 0,
        jnp.broadcast_to(run_cols[rows - 1 : rows, :], (8, LANES)),
        jnp.broadcast_to(run_cols[0:1, :], (8, LANES)),
    )

    def log_copy(flip, who, slot):
        return sending(
            logs.at[slot],
            logs.at[slot],
            log_sems.at[0, flip],
            log_sems.at[1, flip],
            {"sp": base + who},
        )

    flips = (
        spot + 1 - 2 * core,
        lax.rem(spot + 2, CLIQUE),
        CLIQUE - 1 - spot,
    )
    for flip, who in enumerate(flips):
        log_copy(flip, who, spot).start()

    loaded(13)
    rims_do(range(3, 5), "start")

    loaded(16)

    def weight_part(slot, index):
        return weights.at[slot, index]

    def weight_mate(slot):
        return sending(
            weights.at[slot],
            weights.at[slot],
            weight_sems.at[0, 0, 0],
            weight_sems.at[1, 0, 0],
            {"sp": mate},
        )

    def weight_over(index, slot):
        return sending(
            weight_part(slot, index),
            weight_part(slot, index),
            weight_sems.at[0, 1, index],
            weight_sems.at[1, 1, index],
            {"sp": partner},
        )

    def weight_onward(index, slot):
        return sending(
            weight_part(slot, index),
            weight_part(slot, index),
            weight_sems.at[0, 2, index],
            weight_sems.at[1, 2, index],
            {"sp": mate},
        )

    def pass_on(index):
        weight_over(index, flips[1]).wait_recv()
        weight_onward(index, flips[1]).start()


    loaded(10, 11, 12)
    rims_do(range(3), "recv")
    columns = ((src_ref, src_halo, src_taps, xs), (wr_ref, wr_halo, wr_taps, wv), (rd_ref, rd_halo, rd_taps, rv))
    margin = CONV // 2
    for source, halo, taps_ref, target in columns:
        width = source.shape[1]
        taps = taps_ref[...].astype(F32)
        for first in range(0, width, LANES):
            cols = slice(first, first + LANES)
            padded[8 : 8 + rows, :] = source[:, cols].astype(F32)
            padded[0:8, :] = halo[0, :, cols].astype(F32)
            padded[8 + rows : 16 + rows, :] = halo[1, :, cols].astype(F32)
            value = jnp.zeros((rows, LANES), F32)
            for k in range(CONV):
                start = 8 - margin + k
                value = value + padded[start : start + rows, :] * taps[k : k + 1, cols]
            target[:, cols] = silu(value).astype(BF16)

    def own_copy(half, way_up):
        target = layer + (1 if way_up else -1)
        return sending(
            acts.at[half, layer],
            acts.at[half, layer],
            own_sems.at[half, 1 if way_up else 0],
            act_sems.at[1, half, layer],
            at_layer(target),
        )

    part_wide = acts.shape[3]

    def put(half, cols, value):
        first = cols.start
        while first < cols.stop:
            part = first // part_wide
            last = min(cols.stop, (part + 1) * part_wide)
            acts[2 * half + part, layer, :, first - part * part_wide : last - part * part_wide] = value[
                :, first - cols.start : last - cols.start
            ].astype(BF16)
            first = last

    can_up = layer < outer - 1
    can_down = layer > 0

    def own_goes(half, way_up):
        can = can_up if way_up else can_down
        if lean and half >= 2:
            can = can & jnp.logical_not(taker & (buddy == layer + (1 if way_up else -1)))
        return can

    def own_start(half):
        pl.when(own_goes(half, True))(lambda: own_copy(half, True).start())
        pl.when(own_goes(half, False))(lambda: own_copy(half, False).start())

    def far_copy(half, block, sign):
        return sending(
            acts.at[half, block],
            acts.at[half, block],
            act_sems.at[0, half, block],
            act_sems.at[1, half, block],
            at_layer(layer - sign),
        )

    def each(d, do):
        for sign in (-1, 1):
            block = layer + sign * d
            pl.when((block >= 0) & (block < outer))(functools.partial(do, block, sign))

    def relay(half, d):
        def do(block, sign):
            copy = far_copy(half, block, sign)
            copy.wait_recv()
            target = layer - sign
            pl.when((target >= 0) & (target < outer))(lambda: copy.start())

        if half >= 2 and d == 1:
            if_not_giver(lambda: each(d, do))
        else:
            each(d, do)

    groups = wr_ref.shape[1] // STATE
    wide = xs.shape[1]
    group_wide = wide // groups
    per_group = group_wide // SSD_HEAD
    owner = iota((LANES, wide), 1) // SSD_HEAD
    place = iota((LANES, wide), 0)
    pick = []
    for d in range(2):
        hit = (place == owner + 2 * d * gap) | (place == owner + (2 * d + 1) * gap)
        pick.append(jnp.where(hit, 1.0, 0.0).astype(BF16))
    grow_cols = square[1].T.astype(BF16)
    scale_cols = square[2].T.astype(BF16)
    for d in range(2):
        grown[d] = dot(grow_cols, pick[d])
        scaled[d] = (dot(scale_cols, pick[d]) * xs[...].astype(F32)).astype(BF16)
    for g in range(groups):
        cols = slice(g * group_wide, (g + 1) * group_wide)
        write_t = wv[:, g * STATE : (g + 1) * STATE].astype(F32).T.astype(BF16)
        for d in range(2):
            fresh = dot(write_t, scaled[d, :, cols])
            own_state[d, :, cols] = fresh
            state_out[d, :, cols] = fresh.astype(BF16)

    swap = sending(
        state_out.at[1 - way],
        mate_state,
        scan_sems.at[0, 0, 0],
        scan_sems.at[1, 0, 0],
        {"sp": mate},
    )
    swap.start()
    weight_mate(spot).start()

    for flip, who in enumerate(flips):
        log_copy(flip, who, who).wait_recv()
    log_own = logs[spot, pl.ds(way, 1), :]
    log_mate = logs[flips[0], pl.ds(way, 1), :]
    log_partner = logs[flips[1], pl.ds(way, 1), :] + logs[flips[2], pl.ds(way, 1), :]
    log_rows = jnp.where(
        log_row == 0,
        jnp.broadcast_to(log_own, (8, LANES)),
        jnp.where(
            log_row == 1,
            jnp.broadcast_to(log_mate, (8, LANES)),
            jnp.where(
                log_row == 2,
                jnp.broadcast_to(log_partner, (8, LANES)),
                jnp.broadcast_to(log_own + log_mate, (8, LANES)),
            ),
        ),
    )
    high, low = split(jnp.exp(log_rows))
    mine = jnp.where(place == owner + way * gap, 1.0, 0.0).astype(BF16)
    decays[...] = dot(high, mine) + dot(low, mine)
    dec_own = decays[0:1, :]
    dec_mate = decays[1:2, :]
    dec_partner = decays[2:3, :]
    dec_chip = decays[3:4, :]
    dec_layer = dec_partner * dec_chip
    one = jnp.ones_like(dec_own)
    from_partner = jnp.where(later, dec_chip, one)
    from_mine = jnp.where(later, one, dec_partner)
    in_before = jnp.where(later, dec_partner, one)
    in_partner = jnp.where(later, 1.0, 0.0)

    chunk = STATE // CHUNKS

    def over_copy(c):
        part = slice(c * chunk, (c + 1) * chunk)
        return sending(
            total_out.at[part, :],
            partner_total.at[part, :],
            scan_sems.at[0, 1, c],
            scan_sems.at[1, 1, c],
            {"sp": partner},
        )

    def z_copy(c, to):
        part = slice(c * chunk, (c + 1) * chunk)
        return sending(
            z_out.at[part, :],
            z_in.at[part, :],
            scan_sems.at[0, 2, c],
            scan_sems.at[1, 2, c],
            at_layer(to),
        )

    def down_copy(c):
        part = slice(c * chunk, (c + 1) * chunk)
        return sending(
            chip_out.at[part, :],
            incoming.at[way, part, :],
            scan_sems.at[0, 3, c],
            scan_sems.at[1, 3, c],
            {"sp": mate},
        )

    def down_recv(c):
        part = slice(c * chunk, (c + 1) * chunk)
        return sending(
            chip_out.at[part, :],
            incoming.at[1 - way, part, :],
            scan_sems.at[0, 3, c],
            scan_sems.at[1, 3, c],
            {"sp": mate},
        )

    run_at = square[0].T
    causal = iota((rows, rows), 1) <= iota((rows, rows), 0)
    diagonal = iota((rows, rows), 1) == iota((rows, rows), 0)

    def within(g):
        read = rv[:, g * STATE : (g + 1) * STATE]
        write = wv[:, g * STATE : (g + 1) * STATE]
        affinity = dot_t(read, write)
        for j in range(per_group):
            h = g * per_group + j
            cols = slice(h * SSD_HEAD, (h + 1) * SSD_HEAD)
            ahead = run_at[:, h : h + 1] - rows_log[0, h : h + 1, :]
            back = run_at[:, gap + h : gap + h + 1] - rows_log[1, h : h + 1, :]
            fade = jnp.exp(jnp.where(causal, ahead, back))
            length_f = rows_log[2, h : h + 1, :]
            length_b = rows_log[3, h : h + 1, :]
            taken = jnp.where(causal, length_f, length_b) * fade
            taken = taken + jnp.where(diagonal, length_b, 0.0)
            y_sum[:, cols] = dot((affinity * taken).astype(BF16), xs[:, cols])

    for g in range(groups):
        within(g)
    swap.wait_recv()
    for c in range(CHUNKS):
        part = slice(c * chunk, (c + 1) * chunk)
        summed_state = (
            mate_state[part, :].astype(F32) * dec_own + own_state[way, part, :]
        )
        total[part, :] = summed_state
        total_out[part, :] = summed_state.astype(BF16)
        over_copy(c).start()

    rims_do(range(3, 5), "recv")
    loaded(14, 15)
    sharing = q_ref.shape[1] // HEAD // kv_heads
    stacked = (sharing * rows, rows)
    query_at = lax.rem(iota(stacked, 0), rows)
    above = iota(stacked, 1) >= query_at
    below = iota(stacked, 1) <= query_at
    ok_left = above & has_left
    ok_right = below & has_right
    scale = HEAD ** (-0.5)
    for g in range(kv_heads):
        cols = slice(g * HEAD, (g + 1) * HEAD)
        keys = (k_halo[0, :, cols], turned[:, cols], k_halo[1, :, cols])
        values = (v_halo[0, :, cols], v_ref[:, cols], v_halo[1, :, cols])
        first = g * sharing
        query = jnp.concatenate(
            [turn(q_ref[:, h * HEAD : (h + 1) * HEAD]) for h in range(first, first + sharing)], axis=0
        )
        tiles = [dot_t(query, key) * scale for key in keys]
        tiles[0] = jnp.where(ok_left, tiles[0], -jnp.inf)
        tiles[2] = jnp.where(ok_right, tiles[2], -jnp.inf)
        sink = jnp.concatenate(
            [jnp.broadcast_to(sink_ref[:, h : h + 1], (rows, 1)) for h in range(first, first + sharing)],
            axis=0,
        )
        top = jnp.maximum(
            jnp.max(jnp.maximum(jnp.maximum(tiles[0], tiles[1]), tiles[2]), axis=1, keepdims=True),
            sink,
        )
        tiles = [jnp.exp(tile - top) for tile in tiles]
        bottom = jnp.sum(tiles[0] + tiles[1] + tiles[2], axis=1, keepdims=True) + jnp.exp(sink - top)
        inverse = 1.0 / bottom
        found = jnp.zeros((sharing * rows, HEAD), F32)
        for tile, value in zip(tiles, values):
            found = found + dot((tile * inverse).astype(BF16), value)
        for j in range(sharing):
            h = first + j
            put(0, slice(h * HEAD, (h + 1) * HEAD), found[j * rows : (j + 1) * rows])
    own_start(0)
    own_start(1)

    for c in range(CHUNKS):
        part = slice(c * chunk, (c + 1) * chunk)
        over_copy(c).wait_recv()
        level = partner_total[part, :].astype(F32) * from_partner + total[part, :] * from_mine
        total[part, :] = level

        def first_out():
            z_out[part, :] = level.astype(BF16)
            z_copy(c, after).start()

        pl.when(jnp.logical_not(has_before) & has_after)(first_out)
    for index in range(PARTS):
        weight_over(index, spot).start()
    def spare_in(index):
        return sending(
            weights.at[spot, 2 + index],
            spare.at[spot, index],
            spare_sems.at[0, 0, index],
            spare_sems.at[1, 0, index],
            at_layer(buddy),
        )

    def spare_on(kind, index, slot, who):
        return sending(
            spare.at[slot, index],
            spare.at[slot, index],
            spare_sems.at[0, kind, index],
            spare_sems.at[1, kind, index],
            {"sp": who},
        )

    def give_weights():
        for index in range(2):
            spare_in(index).start()

    if_giver(give_weights)

    if outer > 1:
        relay(0, 1)
        relay(1, 1)
    for c in range(CHUNKS):
        part = slice(c * chunk, (c + 1) * chunk)

        def next_out():
            z_copy(c, after).wait_recv()

            def send():
                z_out[part, :] = (
                    z_in[part, :].astype(F32) * dec_layer + total[part, :]
                ).astype(BF16)
                z_copy(c, after).start()

            pl.when(has_after)(send)

        pl.when(has_before)(next_out)
        entering = z_in[part, :].astype(F32)
        chip_in = entering * in_before + partner_total[part, :].astype(F32) * in_partner
        chip_out[part, :] = chip_in.astype(BF16)
        down_copy(c).start()
        incoming[way, part, :] = (
            chip_in * dec_mate + mate_state[part, :].astype(F32)
        ).astype(BF16)
    for d in range(2, outer):
        relay(0, d)
        relay(1, d)
        if d == 2:
            break
    for c in range(CHUNKS):
        down_recv(c).wait_recv()

    loaded(17, 18)
    for g in range(groups):
        cols = slice(g * group_wide, (g + 1) * group_wide)
        read = rv[:, g * STATE : (g + 1) * STATE]
        value = y_sum[:, cols]
        for d in range(2):
            value = value + dot(read, incoming[d, :, cols]) * grown[d, :, cols]
        value = value * silu(gate_ref[:, cols].astype(F32))
        mean = jnp.sum(value * value, axis=1, keepdims=True) * (1.0 / group_wide)
        value = value * lax.rsqrt(mean + EPSILON) * gain_ref[:, cols]
        put(1, cols, value)
    own_start(2)

    share = rows // tps

    def multiply_first(block, sign):
        def body(slot, carry):
            acc[block, slot] = dot(acts[0, block], weights[slot, 0]) + dot(
                acts[1, block], weights[slot, 1]
            )
            return carry

        lax.fori_loop(0, CLIQUE, body, 0)

    def piece_copy(block, part, other, slot):
        span = pl.ds(part * SPLIT, SPLIT)
        return sending(
            partial.at[block, other, span],
            pieces.at[block, slot, span],
            piece_sems.at[0, block, other, part],
            piece_sems.at[1, block, slot, part],
            {"tp": other},
        )

    lanes = [lax.rem(lane + d, tps) for d in range(1, tps)]

    def multiply_third(block, sign):
        def body(slot, carry):
            acc[block, slot] += dot(acts[2, block], weights[slot, 2])
            return carry

        lax.fori_loop(0, CLIQUE, body, 0)

    def multiply_second(block, sign):
        def body(slot, carry):
            product = (acc[block, slot] + dot(acts[3, block], weights[slot, 3])).astype(BF16)
            for other in range(tps):
                partial[block, other, slot] = product[other * share : (other + 1) * share]
            return carry

        for part in range(CLIQUE // SPLIT):
            lax.fori_loop(part * SPLIT, (part + 1) * SPLIT, body, 0)
            for other in lanes:
                piece_copy(block, part, other, lane).start()

    def out_copy(block, slot, part):
        span = pl.ds(part * SPLIT, SPLIT)
        return sending(
            summed.at[block, span],
            landed.at[slot, span],
            out_sems.at[0, block, part],
            out_sems.at[1, slot, part],
            at_layer(block),
        )

    def settle(block, sign):
        for part in range(CLIQUE // SPLIT):
            span = slice(part * SPLIT, (part + 1) * SPLIT)
            result = partial[block, lane, span].astype(F32)
            for other in lanes:
                piece_copy(block, part, other, other).wait_recv()
                result = result + pieces[block, other, span].astype(F32)
            if sign:
                summed[block, span] = result.astype(BF16)
                out_copy(block, layer, part).start()
            else:
                landed[layer, span] = result.astype(BF16)

    weight_mate(flips[0]).wait_recv()
    for index in range(2):
        pass_on(index)
    for index in range(2):
        weight_onward(index, flips[2]).wait_recv()
    multiply_first(layer, 0)
    own_start(3)
    if outer > 1:
        each(1, multiply_first)

    first_copy = sending(
        first_out_sum, first_in_sum, first_sems.at[0], first_sems.at[1], at_layer(buddy)
    )

    def give_first():
        def body(slot, carry):
            first_out_sum[slot] = acc[buddy, slot].astype(BF16)
            return carry

        lax.fori_loop(0, CLIQUE, body, 0)
        first_copy.start()

    if_giver(give_first)
    if outer > 1:
        relay(2, 1)
    for d in range(2, outer):
        if d > 2:
            relay(0, d)
            relay(1, d)
        each(d, multiply_first)
    if outer > 1:
        relay(3, 1)
    if outer > 2:
        relay(2, 2)
    for index in range(2, PARTS):
        pass_on(index)
    for index in range(2, PARTS):
        weight_onward(index, flips[2]).wait_recv()

    def spread_spare():
        for index in range(2):
            spare_in(index).wait_recv()
            spare_on(2, index, spot, partner).start()
            spare_on(1, index, spot, mate).start()

    if_taker(spread_spare)
    def nearest():
        each(1, multiply_third)
        each(1, multiply_second)

    if outer > 1:
        if_not_giver(nearest)
    if outer > 2:
        relay(3, 2)
    if outer > 2:
        each(2, multiply_third)
        each(2, multiply_second)
    multiply_third(layer, 0)
    multiply_second(layer, 0)
    if outer > 1:
        if_not_giver(lambda: each(1, settle))
    for d in range(3, outer):
        relay(2, d)
        each(d, multiply_third)
        relay(3, d)
        each(d, multiply_second)
        each(d - 1, settle)

    def extra_block():
        for index in range(2):
            spare_on(2, index, flips[1], partner).wait_recv()
            spare_on(3, index, flips[1], mate).start()
        first_copy.wait_recv()
        for index in range(2):
            spare_on(1, index, flips[0], mate).wait_recv()
        for index in range(2):
            spare_on(3, index, flips[2], mate).wait_recv()

        def body(slot, carry):
            product = (
                first_in_sum[slot].astype(F32)
                + dot(acts[2, layer], spare[slot, 0])
                + dot(acts[3, layer], spare[slot, 1])
            ).astype(BF16)
            for other in range(tps):
                partial[outer, other, slot] = product[other * share : (other + 1) * share]
            return carry

        for part in range(CLIQUE // SPLIT):
            lax.fori_loop(part * SPLIT, (part + 1) * SPLIT, body, 0)
            for other in lanes:
                piece_copy(outer, part, other, lane).start()

    def extra_settle():
        for part in range(CLIQUE // SPLIT):
            span = slice(part * SPLIT, (part + 1) * SPLIT)
            result = partial[outer, lane, span].astype(F32)
            for other in lanes:
                piece_copy(outer, part, other, other).wait_recv()
                result = result + pieces[outer, other, span].astype(F32)
            landed[buddy, span] = result.astype(BF16)

    if_taker(extra_block)
    if outer > 2:
        each(outer - 1, settle)
    settle(layer, 0)
    if_taker(extra_settle)

    def arrive(block, sign):
        for part in range(CLIQUE // SPLIT):
            out_copy(block, block, part).wait_recv()

    def arrive_near(block, sign):
        if lean:
            pl.when(jnp.logical_not(taker & (block == buddy)))(lambda: arrive(block, sign))
        else:
            arrive(block, sign)

    for d in range(1, outer):
        each(d, arrive_near if d == 1 else arrive)
    width = landed.shape[3]
    for other in range(outer):
        for slot in range(CLIQUE):
            first = (other * CLIQUE + slot) * width
            out_ref[:, first : first + width] = landed[other, slot]

    rims_do(range(5), "send")
    for flip, who in enumerate(flips):
        log_copy(flip, who, spot).wait_send()
    weight_mate(spot).wait_send()
    for half in range(PARTS):
        pl.when(own_goes(half, True))(lambda: own_copy(half, True).wait_send())
        pl.when(own_goes(half, False))(lambda: own_copy(half, False).wait_send())
    for index in range(PARTS):
        weight_over(index, spot).wait_send()
        weight_onward(index, flips[1]).wait_send()
    swap.wait_send()
    for c in range(CHUNKS):
        over_copy(c).wait_send()
        down_copy(c).wait_send()
        pl.when(has_after)(lambda: z_copy(c, after).wait_send())

    def gone(block, sign):
        target = layer - sign
        for half in range(PARTS):
            pl.when((target >= 0) & (target < outer))(
                lambda: far_copy(half, block, sign).wait_send()
            )
        for part in range(CLIQUE // SPLIT):
            out_copy(block, layer, part).wait_send()
            for other in lanes:
                piece_copy(block, part, other, lane).wait_send()

    def given():
        for index in range(2):
            spare_in(index).wait_send()
        first_copy.wait_send()

    def taken():
        for index in range(2):
            spare_on(1, index, spot, mate).wait_send()
            spare_on(2, index, spot, partner).wait_send()
            spare_on(3, index, flips[1], mate).wait_send()
        for part in range(CLIQUE // SPLIT):
            for other in lanes:
                piece_copy(outer, part, other, lane).wait_send()

    if_giver(given)
    if_taker(taken)
    if outer > 1:
        if_not_giver(lambda: each(1, gone))
    for d in range(2, outer):
        each(d, gone)
    for part in range(CLIQUE // SPLIT):
        for other in lanes:
            piece_copy(layer, part, other, lane).wait_send()


def local(
    asking_matrix,
    matching_key_matrix,
    carried_value_matrix,
    silu_switch_argument,
    duality_source_matrix,
    storing_direction_matrix,
    fetching_direction_matrix,
    duality_kernel_coefficients,
    storing_kernel_coefficients,
    fetching_kernel_coefficients,
    raw_increment_lengths,
    logarithmic_fading_speeds,
    token_fading_spikes,
    absorber_score_vector,
    cluster_scaling_factor,
    final_mapping_matrix,
):
    count = lax.axis_size("sp")
    tps = lax.axis_size("tp")
    outer = count // CLIQUE
    rows, q_width = asking_matrix.shape
    k_width = matching_key_matrix.shape[1]
    s_width = duality_source_matrix.shape[1]
    w_width = storing_direction_matrix.shape[1]
    heads = raw_increment_lengths.shape[1]
    width = final_mapping_matrix.shape[2]
    share = rows // tps
    halfway = HEAD // 2
    spacing = ROTARY_BASE ** (-np.arange(halfway, dtype=np.float64) * 2.0 / HEAD)
    spacing = np.concatenate([spacing, spacing])
    angles = np.arange(rows, dtype=np.float64)[:, None] * spacing[None, :]
    firsts = np.arange(count, dtype=np.float64)[:, None] * rows * spacing[None, :]
    turns = np.stack([np.cos(firsts), np.sin(firsts)]).astype(np.float32)
    block = (CLIQUE, share, width)
    return pl.pallas_call(
        functools.partial(mixer_kernel, outer, tps),
        out_shape=jax.ShapeDtypeStruct((share, count * width), BF16),
        in_specs=[pl.BlockSpec(memory_space=pl.ANY)] * 19,
        out_specs=pl.BlockSpec(memory_space=pltpu.VMEM),
        scratch_shapes=[
            pltpu.VMEM((rows, q_width), BF16),
            pltpu.VMEM((rows, k_width), BF16),
            pltpu.VMEM((rows, k_width), BF16),
            pltpu.VMEM((rows, s_width), BF16),
            pltpu.VMEM((rows, s_width), BF16),
            pltpu.VMEM((rows, w_width), BF16),
            pltpu.VMEM((rows, w_width), BF16),
            pltpu.VMEM((CONV, s_width), BF16),
            pltpu.VMEM((CONV, w_width), BF16),
            pltpu.VMEM((CONV, w_width), BF16),
            pltpu.VMEM((2, heads, rows), F32),
            pltpu.VMEM((2, heads), F32),
            pltpu.VMEM((2, heads, rows), F32),
            pltpu.VMEM((1, q_width // HEAD), F32),
            pltpu.VMEM((1, s_width), F32),
            pltpu.VMEM((rows, HEAD), F32),
            pltpu.VMEM((rows, HEAD), F32),
            pltpu.VMEM((2, count, HEAD), F32),
            pltpu.VMEM((rows, k_width), BF16),
            pltpu.VMEM((2, rows, k_width), BF16),
            pltpu.VMEM((2, rows, k_width), BF16),
            pltpu.VMEM((2, TILE, s_width), BF16),
            pltpu.VMEM((2, TILE, w_width), BF16),
            pltpu.VMEM((2, TILE, w_width), BF16),
            pltpu.VMEM((rows + 16, LANES), F32),
            pltpu.VMEM((rows, s_width), BF16),
            pltpu.VMEM((rows, w_width), BF16),
            pltpu.VMEM((rows, w_width), BF16),
            pltpu.VMEM((3, LANES, rows), F32),
            pltpu.VMEM((2, rows, s_width), F32),
            pltpu.VMEM((2, rows, s_width), BF16),
            pltpu.VMEM((4, heads, rows), F32),
            pltpu.VMEM((CLIQUE, 8, LANES), F32),
            pltpu.VMEM((8, s_width), F32),
            pltpu.VMEM((2, STATE, s_width), F32),
            pltpu.VMEM((2, STATE, s_width), BF16),
            pltpu.VMEM((STATE, s_width), BF16),
            pltpu.VMEM((STATE, s_width), F32),
            pltpu.VMEM((STATE, s_width), BF16),
            pltpu.VMEM((STATE, s_width), BF16),
            pltpu.VMEM((STATE, s_width), BF16),
            pltpu.VMEM((STATE, s_width), BF16),
            pltpu.VMEM((STATE, s_width), BF16),
            pltpu.VMEM((2, STATE, s_width), BF16),
            pltpu.VMEM((rows, s_width), F32),
            pltpu.VMEM((PARTS, outer, rows, q_width // 2), BF16),
            pltpu.VMEM((CLIQUE, PARTS, q_width // 2, width), BF16),
            pltpu.VMEM((outer, CLIQUE, rows, width), F32),
            pltpu.VMEM((outer + 1, tps) + block, BF16),
            pltpu.VMEM((outer + 1, tps) + block, BF16),
            pltpu.VMEM((outer,) + block, BF16),
            pltpu.VMEM((outer,) + block, BF16),
            pltpu.VMEM((CLIQUE, 2, q_width // 2, width), BF16),
            pltpu.VMEM((CLIQUE, rows, width), BF16),
            pltpu.VMEM((CLIQUE, rows, width), BF16),
            pltpu.SemaphoreType.DMA((2, 2, 5)),
            pltpu.SemaphoreType.DMA((2, CLIQUE)),
            pltpu.SemaphoreType.DMA((2, 3, PARTS)),
            pltpu.SemaphoreType.DMA((2, 4, CHUNKS)),
            pltpu.SemaphoreType.DMA((2, PARTS, outer)),
            pltpu.SemaphoreType.DMA((PARTS, 2)),
            pltpu.SemaphoreType.DMA((2, outer + 1, tps, CLIQUE // SPLIT)),
            pltpu.SemaphoreType.DMA((2, outer, CLIQUE // SPLIT)),
            pltpu.SemaphoreType.DMA((2, 4, 2)),
            pltpu.SemaphoreType.DMA((2,)),
            pltpu.SemaphoreType.DMA((19,)),
        ],
        compiler_params=pltpu.CompilerParams(collective_id=1, has_side_effects=True),
    )(
        asking_matrix,
        matching_key_matrix,
        carried_value_matrix,
        silu_switch_argument,
        duality_source_matrix,
        storing_direction_matrix,
        fetching_direction_matrix,
        duality_kernel_coefficients,
        storing_kernel_coefficients,
        fetching_kernel_coefficients,
        raw_increment_lengths,
        logarithmic_fading_speeds,
        token_fading_spikes,
        absorber_score_vector.reshape(1, q_width // HEAD),
        cluster_scaling_factor.reshape(1, s_width),
        final_mapping_matrix.reshape(PARTS, q_width // 2, width),
        np.cos(angles).astype(np.float32),
        np.sin(angles).astype(np.float32),
        turns,
    )


def solution(mesh):
    in_specs = (
        P("sp", "tp"),
        P("sp", "tp"),
        P("sp", "tp"),
        P("sp", "tp"),
        P("sp", "tp"),
        P("sp", "tp"),
        P("sp", "tp"),
        P(None, "tp"),
        P(None, "tp"),
        P(None, "tp"),
        P(None, "tp", "sp"),
        P(None, "tp"),
        P(None, "tp", "sp"),
        P("tp"),
        P("tp"),
        P(None, "tp", "sp"),
    )
    out_specs = P(("sp", "tp"), None)
    return jax.shard_map(local, mesh=mesh, in_specs=in_specs, out_specs=out_specs, check_vma=False)
```

```python
import functools

import jax
import jax.numpy as jnp
import numpy as np
from jax import lax
from jax.experimental import pallas as pl
from jax.experimental.pallas import tpu as pltpu
from jax.sharding import PartitionSpec as P

HEAD = 128
SSD_HEAD = 64
STATE = 128
CONV = 5
WINDOW = 128
CLIQUE = 4
TILE = 8
LANES = 128
CHUNKS = 4
PARTS = 4
SPLIT = 2

ROTARY_BASE = 500000.0
EPSILON = 1e-06

F32 = jnp.float32
BF16 = jnp.bfloat16


def sending(source, target, send_sem, recv_sem, partner):
    return pltpu.make_async_remote_copy(
        src_ref=source,
        dst_ref=target,
        send_sem=send_sem,
        recv_sem=recv_sem,
        device_id=partner,
        device_id_type=pl.DeviceIdType.MESH,
    )


def dot(a, b):
    return jnp.dot(a, b, preferred_element_type=F32)


def dot_t(a, b):
    return lax.dot_general(a, b, (((1,), (1,)), ((), ())), preferred_element_type=F32)


def iota(shape, axis):
    return lax.broadcasted_iota(jnp.int32, shape, axis)


def silu(v):
    return v / (1.0 + jnp.exp(-v))


def split(value):
    high = value.astype(BF16)
    return high, (value - high.astype(F32)).astype(BF16)


def mixer_kernel(
    outer,
    tps,
    q_hbm,
    k_hbm,
    v_hbm,
    gate_hbm,
    src_hbm,
    wr_hbm,
    rd_hbm,
    src_taps_hbm,
    wr_taps_hbm,
    rd_taps_hbm,
    inc_hbm,
    fade_hbm,
    spike_hbm,
    sink_hbm,
    gain_hbm,
    weight_hbm,
    cos_hbm,
    sin_hbm,
    base_hbm,
    out_ref,
    q_ref,
    k_ref,
    v_ref,
    gate_ref,
    src_ref,
    wr_ref,
    rd_ref,
    src_taps,
    wr_taps,
    rd_taps,
    inc_ref,
    fade_ref,
    spike_ref,
    sink_ref,
    gain_ref,
    cos_ref,
    sin_ref,
    base_ref,
    turned,
    k_halo,
    v_halo,
    src_halo,
    wr_halo,
    rd_halo,
    padded,
    xs,
    wv,
    rv,
    square,
    grown,
    scaled,
    rows_log,
    logs,
    decays,
    own_state,
    state_out,
    mate_state,
    total,
    total_out,
    partner_total,
    z_out,
    z_in,
    chip_out,
    incoming,
    y_sum,
    acts,
    weights,
    acc,
    partial,
    pieces,
    summed,
    landed,
    spare,
    first_out_sum,
    first_in_sum,
    halo_sems,
    log_sems,
    weight_sems,
    scan_sems,
    act_sems,
    own_sems,
    piece_sems,
    out_sems,
    spare_sems,
    first_sems,
    load_sems,
):
    count = outer * CLIQUE
    rows = q_ref.shape[0]
    me = lax.axis_index("sp")
    lane = lax.axis_index("tp")
    spot = lax.rem(me, CLIQUE)
    layer = me // CLIQUE
    base = me - spot
    core = lax.rem(spot, 2)
    side_y = spot // 2
    mate = base + spot + 1 - 2 * core
    partner = base + lax.rem(spot + 2, CLIQUE)
    across = base + CLIQUE - 1 - spot
    way = 1 - core
    step = 1 - 2 * way
    before = layer - step
    after = layer + step
    has_before = (before >= 0) & (before < outer)
    has_after = (after >= 0) & (after < outer)
    later = (side_y + way) == 1
    has_left = me > 0
    has_right = me < count - 1
    left = {"sp": me - 1}
    right = {"sp": me + 1}

    lean = outer >= 4
    low = (layer < 2).astype(jnp.int32)
    buddy = low * (1 - layer) + (1 - low) * (2 * outer - 3 - layer)
    giver = (layer == 0) | (layer == outer - 1)
    taker = (layer == 1) | (layer == outer - 2)

    def if_giver(do):
        if lean:
            pl.when(giver)(do)

    def if_taker(do):
        if lean:
            pl.when(taker)(do)

    def if_not_giver(do):
        if lean:
            pl.when(jnp.logical_not(giver))(do)
        else:
            do()

    def at_layer(other):
        return {"sp": other * CLIQUE + spot}

    loads = [
        pltpu.make_async_copy(source, target, load_sems.at[index])
        for index, (source, target) in enumerate(
            (
                (base_hbm, base_ref),
                (src_hbm, src_ref),
                (wr_hbm, wr_ref),
                (rd_hbm, rd_ref),
                (k_hbm, k_ref),
                (cos_hbm, cos_ref),
                (sin_hbm, sin_ref),
                (inc_hbm, inc_ref),
                (fade_hbm, fade_ref),
                (spike_hbm, spike_ref),
                (src_taps_hbm, src_taps),
                (wr_taps_hbm, wr_taps),
                (rd_taps_hbm, rd_taps),
                (v_hbm, v_ref),
                (q_hbm, q_ref),
                (sink_hbm, sink_ref),
                (weight_hbm, weights.at[spot]),
                (gate_hbm, gate_ref),
                (gain_hbm, gain_ref),
            )
        )
    ]
    for load in loads:
        load.start()
    barrier = pltpu.get_barrier_semaphore()

    def hail(who):
        pl.semaphore_signal(
            barrier, inc=1, device_id=who, device_id_type=pl.DeviceIdType.MESH
        )

    for other in (mate, partner, across):
        hail({"sp": other})
    for d in range(1, outer):
        hail(at_layer(lax.rem(layer + d, outer)))
    for d in range(1, tps):
        hail({"tp": lax.rem(lane + d, tps)})
    extra_right = (spot == CLIQUE - 1) & has_right
    extra_left = (spot == 0) & has_left
    pl.when(extra_right)(lambda: hail(right))
    pl.when(extra_left)(lambda: hail(left))
    hails = CLIQUE - 1 + outer - 1 + tps - 1

    def loaded(*indices):
        for index in indices:
            loads[index].wait()


    loaded(1, 2, 3)
    pl.semaphore_wait(
        barrier, hails + extra_right.astype(jnp.int32) + extra_left.astype(jnp.int32)
    )

    rims = (
        (src_ref, src_halo, TILE),
        (wr_ref, wr_halo, TILE),
        (rd_ref, rd_halo, TILE),
        (turned, k_halo, rows),
        (v_ref, v_halo, rows),
    )

    def rim_copy(index, to_right):
        source, target, depth = rims[index]
        side = 0 if to_right else 1
        first = rows - depth if to_right else 0
        return sending(
            source.at[first : first + depth, :],
            target.at[side],
            halo_sems.at[0, side, index],
            halo_sems.at[1, side, index],
            right if to_right else left,
        )

    def rims_do(indices, what):
        for index in indices:
            if what == "start":
                pl.when(has_right)(lambda: rim_copy(index, True).start())
                pl.when(has_left)(lambda: rim_copy(index, False).start())
            elif what == "recv":
                pl.when(has_left)(lambda: rim_copy(index, True).wait_recv())
                pl.when(has_right)(lambda: rim_copy(index, False).wait_recv())
            else:
                pl.when(has_right)(lambda: rim_copy(index, True).wait_send())
                pl.when(has_left)(lambda: rim_copy(index, False).wait_send())

    rims_do(range(3), "start")

    def clear(side):
        for _, target, _ in rims:
            target[side] = jnp.zeros(target.shape[1:], target.dtype)

    pl.when(jnp.logical_not(has_left))(lambda: clear(0))
    pl.when(jnp.logical_not(has_right))(lambda: clear(1))

    def clear_in():
        z_in[...] = jnp.zeros_like(z_in)

    pl.when(jnp.logical_not(has_before))(clear_in)

    loaded(0, 4, 5, 6)
    base_cos = base_ref[0, pl.ds(me, 1), :]
    base_sin = base_ref[1, pl.ds(me, 1), :]
    cosine = base_cos * cos_ref[...] - base_sin * sin_ref[...]
    sine = base_sin * cos_ref[...] + base_cos * sin_ref[...]
    sine = jnp.where(iota((rows, HEAD), 1) < HEAD // 2, -sine, sine)

    def turn(block):
        block = block.astype(F32)
        return (block * cosine + pltpu.roll(block, HEAD // 2, 1) * sine).astype(BF16)

    kv_heads = k_ref.shape[1] // HEAD
    for g in range(kv_heads):
        cols = slice(g * HEAD, (g + 1) * HEAD)
        turned[:, cols] = turn(k_ref[:, cols])

    loaded(7, 8, 9)
    heads = inc_ref.shape[1]
    gap = LANES // 4
    lane_at = iota((heads, rows), 1)
    eye = iota((heads, heads), 0) == iota((heads, heads), 1)
    steps = []
    runs = []
    for d in range(2):
        raw = inc_ref[d]
        length = jnp.maximum(raw, 0.0) + jnp.log1p(jnp.exp(-jnp.abs(raw)))
        rate = jnp.sum(
            jnp.where(eye, jnp.broadcast_to(jnp.exp(fade_ref[d : d + 1, :]), (heads, heads)), 0.0),
            axis=1,
            keepdims=True,
        )
        run = spike_ref[d] - rate * length
        hop = 1
        while hop < rows:
            if d == 0:
                moved = jnp.where(lane_at >= hop, pltpu.roll(run, hop, 1), 0.0)
            else:
                moved = jnp.where(lane_at < rows - hop, pltpu.roll(run, rows - hop, 1), 0.0)
            run = run + moved
            hop *= 2
        steps.append(length)
        runs.append(run)
    ends = [runs[0][:, rows - 1 : rows], runs[1][:, 0:1]]
    square[...] = jnp.zeros_like(square)
    for d in range(2):
        square[0, d * gap : d * gap + heads, :] = runs[d]
        fill = jnp.exp(runs[d])
        high = fill.astype(BF16).astype(F32)
        square[1, 2 * d * gap : 2 * d * gap + heads, :] = high
        square[1, (2 * d + 1) * gap : (2 * d + 1) * gap + heads, :] = fill - high
        fill = steps[d] * jnp.exp(ends[d] - runs[d])
        high = fill.astype(BF16).astype(F32)
        square[2, 2 * d * gap : 2 * d * gap + heads, :] = high
        square[2, (2 * d + 1) * gap : (2 * d + 1) * gap + heads, :] = fill - high
        rows_log[d] = runs[d]
        rows_log[2 + d] = steps[d]
    run_cols = square[0].T
    log_row = iota((8, LANES), 0)
    logs[spot] = jnp.where(
        log_row == 0,
        jnp.broadcast_to(run_cols[rows - 1 : rows, :], (8, LANES)),
        jnp.broadcast_to(run_cols[0:1, :], (8, LANES)),
    )

    def log_copy(flip, who, slot):
        return sending(
            logs.at[slot],
            logs.at[slot],
            log_sems.at[0, flip],
            log_sems.at[1, flip],
            {"sp": base + who},
        )

    flips = (
        spot + 1 - 2 * core,
        lax.rem(spot + 2, CLIQUE),
        CLIQUE - 1 - spot,
    )
    for flip, who in enumerate(flips):
        log_copy(flip, who, spot).start()

    loaded(13)
    rims_do(range(3, 5), "start")

    loaded(16)

    def weight_part(slot, index):
        return weights.at[slot, index]

    def weight_mate(slot):
        return sending(
            weights.at[slot],
            weights.at[slot],
            weight_sems.at[0, 0, 0],
            weight_sems.at[1, 0, 0],
            {"sp": mate},
        )

    def weight_over(index, slot):
        return sending(
            weight_part(slot, index),
            weight_part(slot, index),
            weight_sems.at[0, 1, index],
            weight_sems.at[1, 1, index],
            {"sp": partner},
        )

    def weight_onward(index, slot):
        return sending(
            weight_part(slot, index),
            weight_part(slot, index),
            weight_sems.at[0, 2, index],
            weight_sems.at[1, 2, index],
            {"sp": mate},
        )

    def pass_on(index):
        weight_over(index, flips[1]).wait_recv()
        weight_onward(index, flips[1]).start()


    loaded(10, 11, 12)
    rims_do(range(3), "recv")
    columns = ((src_ref, src_halo, src_taps, xs), (wr_ref, wr_halo, wr_taps, wv), (rd_ref, rd_halo, rd_taps, rv))
    margin = CONV // 2
    for source, halo, taps_ref, target in columns:
        width = source.shape[1]
        taps = taps_ref[...].astype(F32)
        for first in range(0, width, LANES):
            cols = slice(first, first + LANES)
            padded[8 : 8 + rows, :] = source[:, cols].astype(F32)
            padded[0:8, :] = halo[0, :, cols].astype(F32)
            padded[8 + rows : 16 + rows, :] = halo[1, :, cols].astype(F32)
            value = jnp.zeros((rows, LANES), F32)
            for k in range(CONV):
                start = 8 - margin + k
                value = value + padded[start : start + rows, :] * taps[k : k + 1, cols]
            target[:, cols] = silu(value).astype(BF16)

    def own_copy(half, way_up):
        target = layer + (1 if way_up else -1)
        return sending(
            acts.at[half, layer],
            acts.at[half, layer],
            own_sems.at[half, 1 if way_up else 0],
            act_sems.at[1, half, layer],
            at_layer(target),
        )

    part_wide = acts.shape[3]

    def put(half, cols, value):
        first = cols.start
        while first < cols.stop:
            part = first // part_wide
            last = min(cols.stop, (part + 1) * part_wide)
            acts[2 * half + part, layer, :, first - part * part_wide : last - part * part_wide] = value[
                :, first - cols.start : last - cols.start
            ].astype(BF16)
            first = last

    can_up = layer < outer - 1
    can_down = layer > 0

    def own_goes(half, way_up):
        can = can_up if way_up else can_down
        if lean and half >= 2:
            can = can & jnp.logical_not(taker & (buddy == layer + (1 if way_up else -1)))
        return can

    def own_start(half):
        pl.when(own_goes(half, True))(lambda: own_copy(half, True).start())
        pl.when(own_goes(half, False))(lambda: own_copy(half, False).start())

    def far_copy(half, block, sign):
        return sending(
            acts.at[half, block],
            acts.at[half, block],
            act_sems.at[0, half, block],
            act_sems.at[1, half, block],
            at_layer(layer - sign),
        )

    def each(d, do):
        for sign in (-1, 1):
            block = layer + sign * d
            pl.when((block >= 0) & (block < outer))(functools.partial(do, block, sign))

    def relay(half, d):
        def do(block, sign):
            copy = far_copy(half, block, sign)
            copy.wait_recv()
            target = layer - sign
            pl.when((target >= 0) & (target < outer))(lambda: copy.start())

        if half >= 2 and d == 1:
            if_not_giver(lambda: each(d, do))
        else:
            each(d, do)

    groups = wr_ref.shape[1] // STATE
    wide = xs.shape[1]
    group_wide = wide // groups
    per_group = group_wide // SSD_HEAD
    owner = iota((LANES, wide), 1) // SSD_HEAD
    place = iota((LANES, wide), 0)
    pick = []
    for d in range(2):
        hit = (place == owner + 2 * d * gap) | (place == owner + (2 * d + 1) * gap)
        pick.append(jnp.where(hit, 1.0, 0.0).astype(BF16))
    grow_cols = square[1].T.astype(BF16)
    scale_cols = square[2].T.astype(BF16)
    for d in range(2):
        grown[d] = dot(grow_cols, pick[d])
        scaled[d] = (dot(scale_cols, pick[d]) * xs[...].astype(F32)).astype(BF16)
    for g in range(groups):
        cols = slice(g * group_wide, (g + 1) * group_wide)
        write_t = wv[:, g * STATE : (g + 1) * STATE].astype(F32).T.astype(BF16)
        for d in range(2):
            fresh = dot(write_t, scaled[d, :, cols])
            own_state[d, :, cols] = fresh
            state_out[d, :, cols] = fresh.astype(BF16)

    swap = sending(
        state_out.at[1 - way],
        mate_state,
        scan_sems.at[0, 0, 0],
        scan_sems.at[1, 0, 0],
        {"sp": mate},
    )
    swap.start()
    weight_mate(spot).start()

    for flip, who in enumerate(flips):
        log_copy(flip, who, who).wait_recv()
    log_own = logs[spot, pl.ds(way, 1), :]
    log_mate = logs[flips[0], pl.ds(way, 1), :]
    log_partner = logs[flips[1], pl.ds(way, 1), :] + logs[flips[2], pl.ds(way, 1), :]
    log_rows = jnp.where(
        log_row == 0,
        jnp.broadcast_to(log_own, (8, LANES)),
        jnp.where(
            log_row == 1,
            jnp.broadcast_to(log_mate, (8, LANES)),
            jnp.where(
                log_row == 2,
                jnp.broadcast_to(log_partner, (8, LANES)),
                jnp.broadcast_to(log_own + log_mate, (8, LANES)),
            ),
        ),
    )
    high, low = split(jnp.exp(log_rows))
    mine = jnp.where(place == owner + way * gap, 1.0, 0.0).astype(BF16)
    decays[...] = dot(high, mine) + dot(low, mine)
    dec_own = decays[0:1, :]
    dec_mate = decays[1:2, :]
    dec_partner = decays[2:3, :]
    dec_chip = decays[3:4, :]
    dec_layer = dec_partner * dec_chip
    one = jnp.ones_like(dec_own)
    from_partner = jnp.where(later, dec_chip, one)
    from_mine = jnp.where(later, one, dec_partner)
    in_before = jnp.where(later, dec_partner, one)
    in_partner = jnp.where(later, 1.0, 0.0)

    chunk = STATE // CHUNKS

    def over_copy(c):
        part = slice(c * chunk, (c + 1) * chunk)
        return sending(
            total_out.at[part, :],
            partner_total.at[part, :],
            scan_sems.at[0, 1, c],
            scan_sems.at[1, 1, c],
            {"sp": partner},
        )

    def z_copy(c, to):
        part = slice(c * chunk, (c + 1) * chunk)
        return sending(
            z_out.at[part, :],
            z_in.at[part, :],
            scan_sems.at[0, 2, c],
            scan_sems.at[1, 2, c],
            at_layer(to),
        )

    def down_copy(c):
        part = slice(c * chunk, (c + 1) * chunk)
        return sending(
            chip_out.at[part, :],
            incoming.at[way, part, :],
            scan_sems.at[0, 3, c],
            scan_sems.at[1, 3, c],
            {"sp": mate},
        )

    def down_recv(c):
        part = slice(c * chunk, (c + 1) * chunk)
        return sending(
            chip_out.at[part, :],
            incoming.at[1 - way, part, :],
            scan_sems.at[0, 3, c],
            scan_sems.at[1, 3, c],
            {"sp": mate},
        )

    run_at = square[0].T
    causal = iota((rows, rows), 1) <= iota((rows, rows), 0)
    diagonal = iota((rows, rows), 1) == iota((rows, rows), 0)

    def within(g):
        read = rv[:, g * STATE : (g + 1) * STATE]
        write = wv[:, g * STATE : (g + 1) * STATE]
        affinity = dot_t(read, write)
        for j in range(per_group):
            h = g * per_group + j
            cols = slice(h * SSD_HEAD, (h + 1) * SSD_HEAD)
            ahead = run_at[:, h : h + 1] - rows_log[0, h : h + 1, :]
            back = run_at[:, gap + h : gap + h + 1] - rows_log[1, h : h + 1, :]
            fade = jnp.exp(jnp.where(causal, ahead, back))
            length_f = rows_log[2, h : h + 1, :]
            length_b = rows_log[3, h : h + 1, :]
            taken = jnp.where(causal, length_f, length_b) * fade
            taken = taken + jnp.where(diagonal, length_b, 0.0)
            y_sum[:, cols] = dot((affinity * taken).astype(BF16), xs[:, cols])

    for g in range(groups):
        within(g)
    swap.wait_recv()
    for c in range(CHUNKS):
        part = slice(c * chunk, (c + 1) * chunk)
        summed_state = (
            mate_state[part, :].astype(F32) * dec_own + own_state[way, part, :]
        )
        total[part, :] = summed_state
        total_out[part, :] = summed_state.astype(BF16)
        over_copy(c).start()

    rims_do(range(3, 5), "recv")
    loaded(14, 15)
    sharing = q_ref.shape[1] // HEAD // kv_heads
    stacked = (sharing * rows, rows)
    query_at = lax.rem(iota(stacked, 0), rows)
    above = iota(stacked, 1) >= query_at
    below = iota(stacked, 1) <= query_at
    ok_left = above & has_left
    ok_right = below & has_right
    scale = HEAD ** (-0.5)
    for g in range(kv_heads):
        cols = slice(g * HEAD, (g + 1) * HEAD)
        keys = (k_halo[0, :, cols], turned[:, cols], k_halo[1, :, cols])
        values = (v_halo[0, :, cols], v_ref[:, cols], v_halo[1, :, cols])
        first = g * sharing
        query = jnp.concatenate(
            [turn(q_ref[:, h * HEAD : (h + 1) * HEAD]) for h in range(first, first + sharing)], axis=0
        )
        tiles = [dot_t(query, key) * scale for key in keys]
        tiles[0] = jnp.where(ok_left, tiles[0], -jnp.inf)
        tiles[2] = jnp.where(ok_right, tiles[2], -jnp.inf)
        sink = jnp.concatenate(
            [jnp.broadcast_to(sink_ref[:, h : h + 1], (rows, 1)) for h in range(first, first + sharing)],
            axis=0,
        )
        top = jnp.maximum(
            jnp.max(jnp.maximum(jnp.maximum(tiles[0], tiles[1]), tiles[2]), axis=1, keepdims=True),
            sink,
        )
        tiles = [jnp.exp(tile - top) for tile in tiles]
        bottom = jnp.sum(tiles[0] + tiles[1] + tiles[2], axis=1, keepdims=True) + jnp.exp(sink - top)
        inverse = 1.0 / bottom
        found = jnp.zeros((sharing * rows, HEAD), F32)
        for tile, value in zip(tiles, values):
            found = found + dot((tile * inverse).astype(BF16), value)
        for j in range(sharing):
            h = first + j
            put(0, slice(h * HEAD, (h + 1) * HEAD), found[j * rows : (j + 1) * rows])
    own_start(0)

    for c in range(CHUNKS):
        part = slice(c * chunk, (c + 1) * chunk)
        over_copy(c).wait_recv()
        level = partner_total[part, :].astype(F32) * from_partner + total[part, :] * from_mine
        total[part, :] = level

        def first_out():
            z_out[part, :] = level.astype(BF16)
            z_copy(c, after).start()

        pl.when(jnp.logical_not(has_before) & has_after)(first_out)
    own_start(1)
    for index in range(PARTS):
        weight_over(index, spot).start()
    def spare_in(index):
        return sending(
            weights.at[spot, 2 + index],
            spare.at[spot, index],
            spare_sems.at[0, 0, index],
            spare_sems.at[1, 0, index],
            at_layer(buddy),
        )

    def spare_on(kind, index, slot, who):
        return sending(
            spare.at[slot, index],
            spare.at[slot, index],
            spare_sems.at[0, kind, index],
            spare_sems.at[1, kind, index],
            {"sp": who},
        )

    def give_weights():
        for index in range(2):
            spare_in(index).start()

    if_giver(give_weights)

    if outer > 1:
        relay(0, 1)
    for c in range(CHUNKS):
        part = slice(c * chunk, (c + 1) * chunk)

        def next_out():
            z_copy(c, after).wait_recv()

            def send():
                z_out[part, :] = (
                    z_in[part, :].astype(F32) * dec_layer + total[part, :]
                ).astype(BF16)
                z_copy(c, after).start()

            pl.when(has_after)(send)

        pl.when(has_before)(next_out)
        entering = z_in[part, :].astype(F32)
        chip_in = entering * in_before + partner_total[part, :].astype(F32) * in_partner
        chip_out[part, :] = chip_in.astype(BF16)
        down_copy(c).start()
        incoming[way, part, :] = (
            chip_in * dec_mate + mate_state[part, :].astype(F32)
        ).astype(BF16)
    if outer > 1:
        relay(1, 1)
    if outer > 2:
        relay(0, 2)
    for c in range(CHUNKS):
        down_recv(c).wait_recv()

    loaded(17, 18)
    for g in range(groups):
        cols = slice(g * group_wide, (g + 1) * group_wide)
        read = rv[:, g * STATE : (g + 1) * STATE]
        value = y_sum[:, cols]
        for d in range(2):
            value = value + dot(read, incoming[d, :, cols]) * grown[d, :, cols]
        value = value * silu(gate_ref[:, cols].astype(F32))
        mean = jnp.sum(value * value, axis=1, keepdims=True) * (1.0 / group_wide)
        value = value * lax.rsqrt(mean + EPSILON) * gain_ref[:, cols]
        put(1, cols, value)
    own_start(2)

    share = rows // tps

    def multiply_first(block, sign):
        def body(slot, carry):
            acc[block, slot] = dot(acts[0, block], weights[slot, 0]) + dot(
                acts[1, block], weights[slot, 1]
            )
            return carry

        lax.fori_loop(0, CLIQUE, body, 0)

    def piece_copy(block, part, other, slot):
        span = pl.ds(part * SPLIT, SPLIT)
        return sending(
            partial.at[block, other, span],
            pieces.at[block, slot, span],
            piece_sems.at[0, block, other, part],
            piece_sems.at[1, block, slot, part],
            {"tp": other},
        )

    lanes = [lax.rem(lane + d, tps) for d in range(1, tps)]

    def multiply_third(block, sign):
        def body(slot, carry):
            acc[block, slot] += dot(acts[2, block], weights[slot, 2])
            return carry

        lax.fori_loop(0, CLIQUE, body, 0)

    def multiply_second(block, sign):
        def body(slot, carry):
            product = (acc[block, slot] + dot(acts[3, block], weights[slot, 3])).astype(BF16)
            for other in range(tps):
                partial[block, other, slot] = product[other * share : (other + 1) * share]
            return carry

        for part in range(CLIQUE // SPLIT):
            lax.fori_loop(part * SPLIT, (part + 1) * SPLIT, body, 0)
            for other in lanes:
                piece_copy(block, part, other, lane).start()

    def out_copy(block, slot, part):
        span = pl.ds(part * SPLIT, SPLIT)
        return sending(
            summed.at[block, span],
            landed.at[slot, span],
            out_sems.at[0, block, part],
            out_sems.at[1, slot, part],
            at_layer(block),
        )

    def settle(block, sign):
        for part in range(CLIQUE // SPLIT):
            span = slice(part * SPLIT, (part + 1) * SPLIT)
            result = partial[block, lane, span].astype(F32)
            for other in lanes:
                piece_copy(block, part, other, other).wait_recv()
                result = result + pieces[block, other, span].astype(F32)
            if sign:
                summed[block, span] = result.astype(BF16)
                out_copy(block, layer, part).start()
            else:
                landed[layer, span] = result.astype(BF16)

    if outer > 2:
        relay(1, 2)
    weight_mate(flips[0]).wait_recv()
    for index in range(2):
        pass_on(index)
    for index in range(2):
        weight_onward(index, flips[2]).wait_recv()
    multiply_first(layer, 0)
    own_start(3)
    if outer > 1:
        each(1, multiply_first)

    first_copy = sending(
        first_out_sum, first_in_sum, first_sems.at[0], first_sems.at[1], at_layer(buddy)
    )

    def give_first():
        def body(slot, carry):
            first_out_sum[slot] = acc[buddy, slot].astype(BF16)
            return carry

        lax.fori_loop(0, CLIQUE, body, 0)
        first_copy.start()

    if_giver(give_first)
    if outer > 1:
        relay(2, 1)
    for d in range(2, outer):
        if d > 2:
            relay(0, d)
            relay(1, d)
        each(d, multiply_first)
    if outer > 1:
        relay(3, 1)
    if outer > 2:
        relay(2, 2)
    for index in range(2, PARTS):
        pass_on(index)
    for index in range(2, PARTS):
        weight_onward(index, flips[2]).wait_recv()

    def spread_spare():
        for index in range(2):
            spare_in(index).wait_recv()
            spare_on(2, index, spot, partner).start()
            spare_on(1, index, spot, mate).start()

    if_taker(spread_spare)
    def nearest():
        each(1, multiply_third)
        each(1, multiply_second)

    if outer > 1:
        if_not_giver(nearest)
    if outer > 2:
        relay(3, 2)
    if outer > 2:
        each(2, multiply_third)
        each(2, multiply_second)
    multiply_third(layer, 0)
    multiply_second(layer, 0)
    if outer > 1:
        if_not_giver(lambda: each(1, settle))
    for d in range(3, outer):
        relay(2, d)
        each(d, multiply_third)
        relay(3, d)
        each(d, multiply_second)
        each(d - 1, settle)

    def extra_block():
        for index in range(2):
            spare_on(2, index, flips[1], partner).wait_recv()
            spare_on(3, index, flips[1], mate).start()
        first_copy.wait_recv()
        for index in range(2):
            spare_on(1, index, flips[0], mate).wait_recv()
        for index in range(2):
            spare_on(3, index, flips[2], mate).wait_recv()

        def body(slot, carry):
            product = (
                first_in_sum[slot].astype(F32)
                + dot(acts[2, layer], spare[slot, 0])
                + dot(acts[3, layer], spare[slot, 1])
            ).astype(BF16)
            for other in range(tps):
                partial[outer, other, slot] = product[other * share : (other + 1) * share]
            return carry

        for part in range(CLIQUE // SPLIT):
            lax.fori_loop(part * SPLIT, (part + 1) * SPLIT, body, 0)
            for other in lanes:
                piece_copy(outer, part, other, lane).start()

    def extra_settle():
        for part in range(CLIQUE // SPLIT):
            span = slice(part * SPLIT, (part + 1) * SPLIT)
            result = partial[outer, lane, span].astype(F32)
            for other in lanes:
                piece_copy(outer, part, other, other).wait_recv()
                result = result + pieces[outer, other, span].astype(F32)
            landed[buddy, span] = result.astype(BF16)

    if_taker(extra_block)
    if outer > 2:
        each(outer - 1, settle)
    settle(layer, 0)
    if_taker(extra_settle)

    def arrive(block, sign):
        for part in range(CLIQUE // SPLIT):
            out_copy(block, block, part).wait_recv()

    def arrive_near(block, sign):
        if lean:
            pl.when(jnp.logical_not(taker & (block == buddy)))(lambda: arrive(block, sign))
        else:
            arrive(block, sign)

    for d in range(1, outer):
        each(d, arrive_near if d == 1 else arrive)
    width = landed.shape[3]
    for other in range(outer):
        for slot in range(CLIQUE):
            first = (other * CLIQUE + slot) * width
            out_ref[:, first : first + width] = landed[other, slot]

    rims_do(range(5), "send")
    for flip, who in enumerate(flips):
        log_copy(flip, who, spot).wait_send()
    weight_mate(spot).wait_send()
    for half in range(PARTS):
        pl.when(own_goes(half, True))(lambda: own_copy(half, True).wait_send())
        pl.when(own_goes(half, False))(lambda: own_copy(half, False).wait_send())
    for index in range(PARTS):
        weight_over(index, spot).wait_send()
        weight_onward(index, flips[1]).wait_send()
    swap.wait_send()
    for c in range(CHUNKS):
        over_copy(c).wait_send()
        down_copy(c).wait_send()
        pl.when(has_after)(lambda: z_copy(c, after).wait_send())

    def gone(block, sign):
        target = layer - sign
        for half in range(PARTS):
            pl.when((target >= 0) & (target < outer))(
                lambda: far_copy(half, block, sign).wait_send()
            )
        for part in range(CLIQUE // SPLIT):
            out_copy(block, layer, part).wait_send()
            for other in lanes:
                piece_copy(block, part, other, lane).wait_send()

    def given():
        for index in range(2):
            spare_in(index).wait_send()
        first_copy.wait_send()

    def taken():
        for index in range(2):
            spare_on(1, index, spot, mate).wait_send()
            spare_on(2, index, spot, partner).wait_send()
            spare_on(3, index, flips[1], mate).wait_send()
        for part in range(CLIQUE // SPLIT):
            for other in lanes:
                piece_copy(outer, part, other, lane).wait_send()

    if_giver(given)
    if_taker(taken)
    if outer > 1:
        if_not_giver(lambda: each(1, gone))
    for d in range(2, outer):
        each(d, gone)
    for part in range(CLIQUE // SPLIT):
        for other in lanes:
            piece_copy(layer, part, other, lane).wait_send()


def local(
    asking_matrix,
    matching_key_matrix,
    carried_value_matrix,
    silu_switch_argument,
    duality_source_matrix,
    storing_direction_matrix,
    fetching_direction_matrix,
    duality_kernel_coefficients,
    storing_kernel_coefficients,
    fetching_kernel_coefficients,
    raw_increment_lengths,
    logarithmic_fading_speeds,
    token_fading_spikes,
    absorber_score_vector,
    cluster_scaling_factor,
    final_mapping_matrix,
):
    count = lax.axis_size("sp")
    tps = lax.axis_size("tp")
    outer = count // CLIQUE
    rows, q_width = asking_matrix.shape
    k_width = matching_key_matrix.shape[1]
    s_width = duality_source_matrix.shape[1]
    w_width = storing_direction_matrix.shape[1]
    heads = raw_increment_lengths.shape[1]
    width = final_mapping_matrix.shape[2]
    share = rows // tps
    halfway = HEAD // 2
    spacing = ROTARY_BASE ** (-np.arange(halfway, dtype=np.float64) * 2.0 / HEAD)
    spacing = np.concatenate([spacing, spacing])
    angles = np.arange(rows, dtype=np.float64)[:, None] * spacing[None, :]
    firsts = np.arange(count, dtype=np.float64)[:, None] * rows * spacing[None, :]
    turns = np.stack([np.cos(firsts), np.sin(firsts)]).astype(np.float32)
    block = (CLIQUE, share, width)
    return pl.pallas_call(
        functools.partial(mixer_kernel, outer, tps),
        out_shape=jax.ShapeDtypeStruct((share, count * width), BF16),
        in_specs=[pl.BlockSpec(memory_space=pl.ANY)] * 19,
        out_specs=pl.BlockSpec(memory_space=pltpu.VMEM),
        scratch_shapes=[
            pltpu.VMEM((rows, q_width), BF16),
            pltpu.VMEM((rows, k_width), BF16),
            pltpu.VMEM((rows, k_width), BF16),
            pltpu.VMEM((rows, s_width), BF16),
            pltpu.VMEM((rows, s_width), BF16),
            pltpu.VMEM((rows, w_width), BF16),
            pltpu.VMEM((rows, w_width), BF16),
            pltpu.VMEM((CONV, s_width), BF16),
            pltpu.VMEM((CONV, w_width), BF16),
            pltpu.VMEM((CONV, w_width), BF16),
            pltpu.VMEM((2, heads, rows), F32),
            pltpu.VMEM((2, heads), F32),
            pltpu.VMEM((2, heads, rows), F32),
            pltpu.VMEM((1, q_width // HEAD), F32),
            pltpu.VMEM((1, s_width), F32),
            pltpu.VMEM((rows, HEAD), F32),
            pltpu.VMEM((rows, HEAD), F32),
            pltpu.VMEM((2, count, HEAD), F32),
            pltpu.VMEM((rows, k_width), BF16),
            pltpu.VMEM((2, rows, k_width), BF16),
            pltpu.VMEM((2, rows, k_width), BF16),
            pltpu.VMEM((2, TILE, s_width), BF16),
            pltpu.VMEM((2, TILE, w_width), BF16),
            pltpu.VMEM((2, TILE, w_width), BF16),
            pltpu.VMEM((rows + 16, LANES), F32),
            pltpu.VMEM((rows, s_width), BF16),
            pltpu.VMEM((rows, w_width), BF16),
            pltpu.VMEM((rows, w_width), BF16),
            pltpu.VMEM((3, LANES, rows), F32),
            pltpu.VMEM((2, rows, s_width), F32),
            pltpu.VMEM((2, rows, s_width), BF16),
            pltpu.VMEM((4, heads, rows), F32),
            pltpu.VMEM((CLIQUE, 8, LANES), F32),
            pltpu.VMEM((8, s_width), F32),
            pltpu.VMEM((2, STATE, s_width), F32),
            pltpu.VMEM((2, STATE, s_width), BF16),
            pltpu.VMEM((STATE, s_width), BF16),
            pltpu.VMEM((STATE, s_width), F32),
            pltpu.VMEM((STATE, s_width), BF16),
            pltpu.VMEM((STATE, s_width), BF16),
            pltpu.VMEM((STATE, s_width), BF16),
            pltpu.VMEM((STATE, s_width), BF16),
            pltpu.VMEM((STATE, s_width), BF16),
            pltpu.VMEM((2, STATE, s_width), BF16),
            pltpu.VMEM((rows, s_width), F32),
            pltpu.VMEM((PARTS, outer, rows, q_width // 2), BF16),
            pltpu.VMEM((CLIQUE, PARTS, q_width // 2, width), BF16),
            pltpu.VMEM((outer, CLIQUE, rows, width), F32),
            pltpu.VMEM((outer + 1, tps) + block, BF16),
            pltpu.VMEM((outer + 1, tps) + block, BF16),
            pltpu.VMEM((outer,) + block, BF16),
            pltpu.VMEM((outer,) + block, BF16),
            pltpu.VMEM((CLIQUE, 2, q_width // 2, width), BF16),
            pltpu.VMEM((CLIQUE, rows, width), BF16),
            pltpu.VMEM((CLIQUE, rows, width), BF16),
            pltpu.SemaphoreType.DMA((2, 2, 5)),
            pltpu.SemaphoreType.DMA((2, CLIQUE)),
            pltpu.SemaphoreType.DMA((2, 3, PARTS)),
            pltpu.SemaphoreType.DMA((2, 4, CHUNKS)),
            pltpu.SemaphoreType.DMA((2, PARTS, outer)),
            pltpu.SemaphoreType.DMA((PARTS, 2)),
            pltpu.SemaphoreType.DMA((2, outer + 1, tps, CLIQUE // SPLIT)),
            pltpu.SemaphoreType.DMA((2, outer, CLIQUE // SPLIT)),
            pltpu.SemaphoreType.DMA((2, 4, 2)),
            pltpu.SemaphoreType.DMA((2,)),
            pltpu.SemaphoreType.DMA((19,)),
        ],
        compiler_params=pltpu.CompilerParams(collective_id=1, has_side_effects=True),
    )(
        asking_matrix,
        matching_key_matrix,
        carried_value_matrix,
        silu_switch_argument,
        duality_source_matrix,
        storing_direction_matrix,
        fetching_direction_matrix,
        duality_kernel_coefficients,
        storing_kernel_coefficients,
        fetching_kernel_coefficients,
        raw_increment_lengths,
        logarithmic_fading_speeds,
        token_fading_spikes,
        absorber_score_vector.reshape(1, q_width // HEAD),
        cluster_scaling_factor.reshape(1, s_width),
        final_mapping_matrix.reshape(PARTS, q_width // 2, width),
        np.cos(angles).astype(np.float32),
        np.sin(angles).astype(np.float32),
        turns,
    )


def solution(mesh):
    in_specs = (
        P("sp", "tp"),
        P("sp", "tp"),
        P("sp", "tp"),
        P("sp", "tp"),
        P("sp", "tp"),
        P("sp", "tp"),
        P("sp", "tp"),
        P(None, "tp"),
        P(None, "tp"),
        P(None, "tp"),
        P(None, "tp", "sp"),
        P(None, "tp"),
        P(None, "tp", "sp"),
        P("tp"),
        P("tp"),
        P(None, "tp", "sp"),
    )
    out_specs = P(("sp", "tp"), None)
    return jax.shard_map(local, mesh=mesh, in_specs=in_specs, out_specs=out_specs, check_vma=False)
```
